32 devices in a mesh: grp: 2 (over y), fs: 4 (over z), tp: 4 (over x, core).
Axes of the slice: x: 2, y: 2, z: 4, core: 2. Of those that a mesh axis runs over, the one named last changes fastest.
Arguments:
- tokens: bfloat16 [4096, 2048], P(('grp', 'fs'), 'tp'), parts along dimension 0, may hold values from -36 to 36
- query_matrix: bfloat16 [2048, 1024], P('fs', 'tp'), may hold values from -0.125 to 0.125
- key_weight: bfloat16 [2048, 1024], P('fs', 'tp'), may hold values from -0.125 to 0.125
- value_weight: bfloat16 [2048, 2048], P('fs', 'tp'), may hold values from -0.125 to 0.125
- forget_lower_factor: bfloat16 [2048, 32], replicated, may hold values from -0.125 to 0.125
- decay_up: bfloat16 [32, 1024], replicated, may hold values from -1 to 1
- decay_bias: float32 [1024], replicated, may hold values from -1 to 8
- log_extra: float32 [4096, 1024], P(('grp', 'fs'), 'tp'), parts along dimension 0, may hold values from -0.7 to 0
- head_gain: float32 [256], replicated, may hold values from 0.1 to 1.9
- out_weight: bfloat16 [2048, 2048], P('tp', 'fs'), may hold values from -0.125 to 0.125
- mix_gain: float32 [2048], P('tp'), may hold values from 0.1 to 1.9
- up_weight: bfloat16 [2048, 8192], P('fs', 'tp'), may hold values from -0.125 to 0.125
- down_weight: bfloat16 [8192, 2048], P('tp', 'fs'), may hold values from -0.0625 to 0.0625
- out_gain: float32 [2048], P('tp'), may hold values from 0.1 to 1.9
Outputs:
- layer_out: bfloat16 [4096, 2048], P(('grp', 'fs'), 'tp'), parts along dimension 0
The draws below stay inside these ranges and needn't reach their ends.
There are 2 independent parts, one for each index of `grp`. The reference program is written for one: setup_inputs(seed, part) draws one part's arguments, and reference() takes and returns one part's arrays. A program takes and returns all parts, laid end to end along the dimension named above; an argument that names none is the same for every part. Nothing has to cross between parts.
All inputs are finite; a program needn't handle non-finite values.
Results may differ from the reference program's by a relative error of at most 0.015.
Values may be sent and summed in bfloat16 or wider, within the bound.
A program may use at most 64 MiB of HBM per device.

```python
import math
import jax
import jax.numpy as jnp
from jax import lax

D = 2048
HEADS = 8
DK = 128
DV = 256
FF = 8192
RANK = 32
SEGMENT_LENGTH = 64
SEQ = 512
OVERALL_WORDS = 2048
N_TP = 4


def draw_tokens(key, part):
    address_embeddings = jax.random.split(key, 3)
    column_index = jnp.arange(D).astype(jnp.float32)
    col_scale = 3.0 ** (column_index / (D - 1)) * jnp.exp(jax.random.uniform(address_embeddings[1], (D,), jnp.float32, 0.0, math.log(1.5))) / 1.5
    row_scale = jnp.exp(jax.random.uniform(address_embeddings[2], (OVERALL_WORDS, 1), jnp.float32, 0.0, math.log(2.0)))
    base = jnp.clip(jax.random.normal(address_embeddings[0], (OVERALL_WORDS, D), jnp.float32), -6.0, 6.0)
    return (base * col_scale * row_scale).astype(jnp.bfloat16)


def draw_decay_bias(key, part):
    address_embeddings = jax.random.split(key, 3)
    width = HEADS * DK
    picked = jax.random.randint(address_embeddings[0], (width,), 0, 2)
    fast = jax.random.uniform(address_embeddings[1], (width,), jnp.float32, -1.0, 1.5)
    slow = jax.random.uniform(address_embeddings[2], (width,), jnp.float32, 4.0, 7.0)
    return jnp.where(picked == 1, fast, slow)


def draw_log_extra(key, part):
    address_embeddings = jax.random.split(key, 3)
    width = HEADS * DK
    forget_speeds = jnp.exp(jax.random.uniform(address_embeddings[0], (OVERALL_WORDS // SEGMENT_LENGTH, width), jnp.float32, math.log(0.0005), math.log(0.004)))
    word_segments = jax.random.randint(address_embeddings[1], (OVERALL_WORDS, 1), 0, 128) == 0
    forget_intensity = jax.random.uniform(address_embeddings[2], (OVERALL_WORDS, width), jnp.float32, math.log(0.5), math.log(0.8))
    return -jnp.repeat(forget_speeds, SEGMENT_LENGTH, axis=0) + jnp.where(word_segments, forget_intensity, 0.0)


def block_levels(stream_key, dims, cuts, low, high):
    level, own = 1.0, jax.random.fold_in(stream_key, 6)
    for axis_at, shards_of in cuts:
        heights = jnp.exp(jax.random.uniform(jax.random.fold_in(own, axis_at), (shards_of,), jnp.float32, low / len(cuts), high / len(cuts)))
        level = level * jnp.repeat(heights, dims[axis_at] // shards_of).reshape([-1 if axis == axis_at else 1 for axis in range(len(dims))])
    return level


def noise(stream_key, shape, scale, bound, cuts=(), dtype=jnp.bfloat16):
    values = scale * jax.random.normal(stream_key, shape, jnp.float32)
    if cuts:
        values = values * block_levels(stream_key, shape, cuts, -0.22, 0.18)
    return jnp.clip(values, -bound, bound).astype(dtype)


def setup_inputs(seed: int = 0, part: int = 0) -> dict:
    keys = jax.random.split(jax.random.key(seed), 15)
    part_keys = jax.random.split(jax.random.fold_in(keys[14], part), 15)
    tokens = draw_tokens(jax.random.fold_in(jax.random.fold_in(keys[14], part), 71), part)
    query_matrix = noise(keys[1], (D, HEADS * DK), D ** -0.5, 0.125, ((0, 4), (1, 4)))
    key_weight = noise(keys[2], (D, HEADS * DK), D ** -0.5, 0.125, ((0, 4), (1, 4)))
    value_weight = noise(keys[3], (D, HEADS * DV), D ** -0.5, 0.125, ((0, 4), (1, 4)))
    forget_lower_factor = noise(keys[4], (D, RANK), D ** -0.5, 0.125)
    decay_up = noise(keys[5], (RANK, HEADS * DK), RANK ** -0.5, 1.0)
    decay_bias = draw_decay_bias(jax.random.fold_in(keys[14], 71), part)
    log_extra = draw_log_extra(jax.random.fold_in(jax.random.fold_in(keys[14], part), 71), part)
    head_gain = jnp.clip(1.0 + 0.18 * jax.random.normal(keys[8], (DV,), jnp.float32), 0.1, 1.9)
    out_weight = noise(keys[9], (HEADS * DV, D), (HEADS * DV) ** -0.5, 0.125, ((0, 4), (1, 4)))
    mix_gain = jnp.clip(1.0 + 0.18 * jax.random.normal(keys[10], (D,), jnp.float32), 0.1, 1.9)
    up_weight = noise(keys[11], (D, FF), D ** -0.5, 0.125, ((0, 4), (1, 4)))
    down_weight = noise(keys[12], (FF, D), FF ** -0.5, 0.0625, ((0, 4), (1, 4)))
    out_gain = jnp.clip(1.0 + 0.18 * jax.random.normal(keys[13], (D,), jnp.float32), 0.1, 1.9)
    return {"tokens": tokens, "query_matrix": query_matrix, "key_weight": key_weight, "value_weight": value_weight, "forget_lower_factor": forget_lower_factor, "decay_up": decay_up, "decay_bias": decay_bias, "log_extra": log_extra, "head_gain": head_gain, "out_weight": out_weight, "mix_gain": mix_gain, "up_weight": up_weight, "down_weight": down_weight, "out_gain": out_gain}


ALPHA = 2.0 ** 0.5
TAU = 16.0
EPS = 1e-05
HIGH = lax.Precision.HIGHEST

def block_scan(queries, key_rows, value_rows, log_decay):
    span = queries.shape[2]
    causal = (jnp.arange(span)[:, None] >= jnp.arange(span)[None, :])[:, :, None]

    def step(state, inputs):
        query_block, key_block, value_block, decay_block = inputs
        cumul = jnp.cumsum(decay_block, axis=1)
        last_cum = cumul[:, -1:, :]
        carried = jnp.einsum('hcd,hde->hce', query_block * jnp.exp(cumul), state, precision=HIGH)
        differ = cumul[:, :, None, :] - cumul[:, None, :, :]
        weights = jnp.exp(jnp.where(causal, differ, -jnp.inf))
        scores = lax.optimization_barrier(jnp.sum(query_block[:, :, None, :] * key_block[:, None, :, :] * weights, axis=-1))
        within = jnp.einsum('hij,hje->hie', scores, value_block, precision=HIGH)
        fresh = jnp.einsum('hcd,hce->hde', key_block * jnp.exp(last_cum - cumul), value_block, precision=HIGH)
        new_state = jnp.exp(last_cum[:, 0, :])[:, :, None] * state + fresh
        return (new_state, carried + within)
    start = jnp.zeros((queries.shape[1], queries.shape[3], value_rows.shape[3]), jnp.float32)
    _, outputs = lax.scan(step, start, (queries, key_rows, value_rows, log_decay))
    return outputs

def mixer_sequence(inputs):
    queries, key_rows, value_rows, log_decay = inputs
    count = queries.shape[0] // SEGMENT_LENGTH

    def blocks(array, depth):
        return array.astype(jnp.float32).reshape(count, SEGMENT_LENGTH, HEADS, depth).transpose(0, 2, 1, 3)
    outputs = block_scan(blocks(queries, DK) * DK ** (-0.5), blocks(key_rows, DK), blocks(value_rows, DV), blocks(log_decay, DK))
    return outputs.transpose(0, 2, 1, 3).reshape(queries.shape[0], HEADS, DV)

def group_sum(left, right, width):
    running = jnp.zeros((left.shape[0], right.shape[1]), jnp.float32)
    for index in range(N_TP):
        partial_sum = jnp.dot(left[:, index * width:(index + 1) * width], right[index * width:(index + 1) * width], preferred_element_type=jnp.float32).astype(jnp.bfloat16)
        partial_sum = lax.optimization_barrier(partial_sum)
        running = running + partial_sum.astype(jnp.float32)
    return running

def layer_norm(summed, gain_cols):
    row_mean = lax.optimization_barrier(jnp.mean(summed, axis=1, keepdims=True))
    centered = summed - row_mean
    row_var = lax.optimization_barrier(jnp.mean(centered * centered, axis=1, keepdims=True))
    return (centered * lax.rsqrt(row_var + EPS) * gain_cols).astype(jnp.bfloat16)

def reference(tokens, query_matrix, key_weight, value_weight, forget_lower_factor, decay_up, decay_bias, log_extra, head_gain, out_weight, mix_gain, up_weight, down_weight, out_gain):
    queries = jnp.dot(tokens, query_matrix, preferred_element_type=jnp.float32).astype(jnp.bfloat16)
    key_rows = jnp.dot(tokens, key_weight, preferred_element_type=jnp.float32).astype(jnp.bfloat16)
    value_rows = jnp.dot(tokens, value_weight, preferred_element_type=jnp.float32).astype(jnp.bfloat16)
    low = jnp.dot(tokens, forget_lower_factor, preferred_element_type=jnp.float32).astype(jnp.bfloat16)
    gate_pre = jnp.dot(low, decay_up, preferred_element_type=jnp.float32) + decay_bias
    log_decay = jax.nn.log_sigmoid(gate_pre) / TAU + log_extra
    count = tokens.shape[0] // SEQ
    attended = lax.map(mixer_sequence, (queries.reshape(count, SEQ, HEADS * DK), key_rows.reshape(count, SEQ, HEADS * DK), value_rows.reshape(count, SEQ, HEADS * DV), log_decay.reshape(count, SEQ, HEADS * DK)))
    attended = attended.reshape(tokens.shape[0], HEADS, DV)
    scaled = attended * lax.rsqrt(lax.optimization_barrier(jnp.mean(attended * attended, axis=-1, keepdims=True)) + EPS) * head_gain
    mixed_heads = scaled.reshape(tokens.shape[0], HEADS * DV).astype(jnp.bfloat16)
    mix = group_sum(mixed_heads, out_weight, HEADS * DV // N_TP)
    normed = layer_norm(ALPHA * tokens.astype(jnp.float32) + mix, mix_gain)
    hidden = jnp.dot(normed, up_weight, preferred_element_type=jnp.float32)
    activation = jnp.square(jax.nn.relu(hidden)).astype(jnp.bfloat16)
    down = group_sum(activation, down_weight, FF // N_TP)
    return layer_norm(ALPHA * normed.astype(jnp.float32) + down, out_gain)
```

```python
import functools

import jax
import jax.numpy as jnp
from jax import lax
from jax.experimental import pallas as pl
from jax.experimental.pallas import tpu as pltpu
from jax.sharding import PartitionSpec as P

DK = 128
DV = 256
CHUNK = 64
SUB = 16
TILE = 256
BAND = 128

ALPHA = 2.0**0.5
TAU = 16.0
EPS = 1e-05

MESH = pl.DeviceIdType.MESH
NT = (((1,), (1,)), ((), ()))
TN = (((0,), (0,)), ((), ()))
BF16, F32 = jnp.bfloat16, jnp.float32


def dot(a, b):
    return jnp.dot(a, b, preferred_element_type=F32)


def loop(count, size, body):
    def step(index, carry):
        body(pl.ds(pl.multiple_of(index * size, size), size))
        return carry

    lax.fori_loop(0, count // size, step, 0)


def when(cond, body):
    if cond is None:
        body()
    else:
        pl.when(cond)(body)


class Sends:
    def __init__(self):
        self.open = []

    def start(self, src, dst, send, recv, device, cond=None):
        def copy():
            return pltpu.make_async_remote_copy(
                src_ref=src, dst_ref=dst, send_sem=send, recv_sem=recv,
                device_id=device, device_id_type=MESH,
            )

        when(cond, lambda: copy().start())
        self.open.append((cond, copy))

    def drain(self):
        for cond, copy in self.open:
            when(cond, lambda copy=copy: copy().wait_send())
        self.open = []


def scan_heads(heads, qkv_ref, decay_ref, gain, out_ref, events):
    rows = qkv_ref.shape[0]
    at_row = lax.broadcasted_iota(jnp.int32, (CHUNK, CHUNK), 0)
    at_col = lax.broadcasted_iota(jnp.int32, (CHUNK, CHUNK), 1)
    tri = (at_row >= at_col).astype(F32)
    sub_row = lax.broadcasted_iota(jnp.int32, (SUB, SUB), 0)
    sub_col = lax.broadcasted_iota(jnp.int32, (SUB, SUB), 1)

    def step(index, states):
        for at, event in events:
            pl.when(index == at)(event)
        here = pl.ds(pl.multiple_of(index * CHUNK, CHUNK), CHUNK)
        fresh_states = []
        for head in range(heads):
            query = qkv_ref[here, head * DK : (head + 1) * DK].astype(F32) * DK**-0.5
            keys = qkv_ref[here, (heads + head) * DK : (heads + head + 1) * DK].astype(F32)
            at_value = 2 * heads * DK + head * DV
            value = qkv_ref[here, at_value : at_value + DV]
            decay = decay_ref[here, head * DK : (head + 1) * DK]
            cumul = jnp.dot(
                tri, decay, precision=lax.Precision.HIGHEST, preferred_element_type=F32
            )
            last = cumul[CHUNK - 1 : CHUNK, :]
            state = states[head]
            out = lax.dot_general(
                (query * jnp.exp(cumul)).astype(BF16),
                state.astype(BF16),
                NT,
                preferred_element_type=F32,
            )
            strips = []
            for a in range(CHUNK // SUB):
                lo, hi = a * SUB, (a + 1) * SUB
                q_a, k_a, g_a = query[lo:hi], keys[lo:hi], cumul[lo:hi]
                diag = jnp.zeros((SUB, SUB), F32)
                for j in range(SUB):
                    weight = jnp.exp(jnp.minimum(g_a - g_a[j : j + 1], 0.0))
                    column = jnp.sum(q_a * k_a[j : j + 1] * weight, axis=1, keepdims=True)
                    diag = jnp.where((sub_col == j) & (sub_row >= j), column, diag)
                strip = dot(diag.astype(BF16), value[lo:hi])
                if a:
                    base = cumul[lo - 1 : lo]
                    before = lax.dot_general(
                        (q_a * jnp.exp(g_a - base)).astype(BF16),
                        (keys[:lo] * jnp.exp(base - cumul[:lo])).astype(BF16),
                        NT,
                        preferred_element_type=F32,
                    )
                    strip += dot(before.astype(BF16), value[:lo])
                strips.append(strip)
            out = out + jnp.concatenate(strips, axis=0)
            fresh = lax.dot_general(
                value,
                (keys * jnp.exp(last - cumul)).astype(BF16),
                TN,
                preferred_element_type=F32,
            )
            fresh_states.append(state * jnp.exp(last) + fresh)
            mean = jnp.mean(out * out, axis=1, keepdims=True)
            out_ref[here, head * DV : (head + 1) * DV] = (
                out * lax.rsqrt(mean + EPS) * gain
            ).astype(BF16)
        return tuple(fresh_states)

    start = tuple(jnp.zeros((DV, DK), F32) for _ in range(heads))
    lax.fori_loop(0, rows // CHUNK, step, start)


def kernel(
    F, T,
    tokens, query, key, value, lower, decay_up, decay_bias, extra, head_gain, out_weight,
    mix_gain, up, down, out_gain,
    result,
    tokg, wqkv, wout, wup, wdown, qkv, decay, mixed, mp, md, xs, xr, mk, v, st, sta, normg, act,
    dnp, dnd, ck, dzs, dzr, dxs, dxr,
    loc, tok_s, tok_r, qz_s, qz_r, qy_s, qy_r, oz_s, oz_r, oy_s, oy_r, uz_s, uz_r, uy_s, uy_r,
    dz_s, dz_r, dy_s, dy_r, md_s, md_r, mx_s, mx_r, st_s, st_r, nm_s, nm_r, dd_s, dd_r,
    dp_s, dp_r, dx_s, dx_r,
):
    U, X = F // T, T // 2
    R, Co = v.shape[1], v.shape[2]
    Rz, W = wqkv.shape[1], wqkv.shape[2]
    kc, vc = query.shape[1], value.shape[1]
    Ko, FH = wout.shape[1], wup.shape[2]
    S = qz_s.shape[2]
    S2 = uz_s.shape[1]
    heads = kc // DK
    g, z, t = lax.axis_index("grp"), lax.axis_index("fs"), lax.axis_index("tp")
    x, c = lax.div(t, 2), lax.rem(t, 2)
    h = lax.rem(z, 2)
    mate = z + 1 - 2 * h
    sends = Sends()

    at_z = lambda other: (g, other, t)
    at_t = lambda other: (g, z, other)
    at_y = (1 - g, z, t)
    at_core = (g, z, t + 1 - 2 * c)
    core = t + 1 - 2 * c

    def arrived(dst, sem, cond=None):
        when(cond, lambda: pltpu.make_async_remote_copy(
            src_ref=dst, dst_ref=dst, send_sem=sem, recv_sem=sem,
            device_id=at_y, device_id_type=MESH,
        ).wait_recv())

    def aligned(value, size):
        return pl.multiple_of(value * size, size)

    copies = [
        pltpu.make_async_copy(query, wqkv.at[z, :, pl.ds(0, kc)], loc.at[0]),
        pltpu.make_async_copy(key, wqkv.at[z, :, pl.ds(kc, kc)], loc.at[1]),
        pltpu.make_async_copy(value, wqkv.at[z, :, pl.ds(2 * kc, vc)], loc.at[2]),
    ]
    tok_copies = [
        pltpu.make_async_copy(tokens.at[:, pl.ds(u * Co, Co)], tokg.at[t * U + u], loc.at[3 + u])
        for u in range(U)
    ]
    late_copies = [
        pltpu.make_async_copy(out_weight, wout.at[z], loc.at[3 + U]),
        pltpu.make_async_copy(up.at[:, pl.ds(aligned(h, FH), FH)], wup.at[z], loc.at[4 + U]),
        pltpu.make_async_copy(down.at[pl.ds(aligned(h, FH), FH), :], wdown.at[z], loc.at[5 + U]),
    ]
    for copy in copies + tok_copies + late_copies:
        copy.start()

    barrier = pltpu.get_barrier_semaphore()
    partners = [at_y]
    partners += [at_z(lax.rem(z + i, F)) for i in range(1, F)]
    partners += [at_t(lax.rem(t + i, T)) for i in range(1, T)]
    for device in partners:
        pl.semaphore_signal(barrier, inc=1, device_id=device, device_id_type=MESH)
    pl.semaphore_wait(barrier, len(partners))

    half = Rz // 2
    step = half // S

    def piece(owner, s, side):
        return wqkv.at[owner, pl.ds(pl.multiple_of(side * half + s * step, step), step), :]

    for copy in copies:
        copy.wait()
    for s in range(S):
        for way, cond in ((0, z < F - 1), (1, z > 0)):
            to = z + 1 - 2 * way
            sends.start(piece(z, s, g), piece(z, s, g), qz_s.at[way, z, s], qz_r.at[z, s], at_z(to), cond)
    for copy in tok_copies:
        copy.wait()
    for i in range(1, T):
        to = lax.rem(t + i, T)
        mine = tokg.at[pl.ds(t * U, U)]
        sends.start(mine, mine, tok_s.at[to], tok_r.at[t], at_t(to))
    for d in range(1, F):
        for s in range(S):
            for way in (0, 1):
                owner = z - d if way == 0 else z + d
                there = z >= d if way == 0 else z + d < F
                onward = (z >= d) & (z < F - 1) if way == 0 else (z + d < F) & (z > 0)
                to = z + 1 - 2 * way
                mine = piece(owner, s, g)
                arrived(mine, qz_r.at[owner, s], there)
                sends.start(mine, mine, qz_s.at[way, owner, s], qz_r.at[owner, s], at_z(to), onward)
                sends.start(mine, mine, qy_s.at[owner, s], qy_r.at[owner, s], at_y, there)

    for copy in late_copies:
        copy.wait()

    def out_piece(owner, side):
        return wout.at[owner, pl.ds(aligned(side, Ko // 2), Ko // 2), :]

    def up_piece(owner, s, side):
        size = Rz // 2 // S2
        return wup.at[owner, pl.ds(pl.multiple_of(side * (Rz // 2) + s * size, size), size), :]

    def down_piece(owner, s, side):
        size = FH // 2 // S2
        return wdown.at[owner, pl.ds(pl.multiple_of(side * (FH // 2) + s * size, size), size), :]

    for i in range(1, F):
        to = lax.rem(z + i, F)
        sends.start(out_piece(z, g), out_piece(z, g), oz_s.at[to], oz_r.at[z], at_z(to))
    for i in range(1, F):
        to = lax.rem(z + i, F)
        part = lax.rem(to, 2)
        size = Rz // 2 // S2
        for s in range(S2):
            rows = pl.ds(pl.multiple_of(g * (Rz // 2) + s * size, size), size)
            sends.start(
                up.at[rows, pl.ds(aligned(part, FH), FH)], up_piece(z, s, g),
                uz_s.at[to, s], uz_r.at[z, s], at_z(to),
            )
    for i in range(1, F):
        to = lax.rem(z + i, F)
        part = lax.rem(to, 2)
        size = FH // 2 // S2
        for s in range(S2):
            rows = pl.ds(pl.multiple_of(part * FH + g * (FH // 2) + s * size, size), size)
            sends.start(
                down.at[rows, :], down_piece(z, s, g), dz_s.at[to, s], dz_r.at[z, s], at_z(to),
            )

    def pass_on(make, z_sem, y_send, y_recv):
        mine = make(g)
        arrived(mine, z_sem)
        sends.start(mine, mine, y_send, y_recv, at_y)

    def out_event(i):
        owner = lax.rem(z + F - i, F)
        mine = out_piece(owner, g)
        here, send, recv = oz_r.at[owner], oy_s.at[owner], oy_r.at[owner]

        def event():
            arrived(mine, here)
            sends.start(mine, mine, send, recv, at_y)

        return event

    def up_event(i, s):
        owner = lax.rem(z + F - i, F)
        pass_on(lambda side: up_piece(owner, s, side), uz_r.at[owner, s], uy_s.at[owner, s], uy_r.at[owner, s])

    def down_event(i, s):
        owner = lax.rem(z + F - i, F)
        pass_on(lambda side: down_piece(owner, s, side), dz_r.at[owner, s], dy_s.at[owner, s], dy_r.at[owner, s])

    for i in range(1, T):
        owner = lax.rem(t + i, T)
        arrived(tokg.at[pl.ds(owner * U, U)], tok_r.at[owner])
    local_up = decay_up[:, pl.ds(aligned(t, kc), kc)]
    local_bias = decay_bias[:, pl.ds(aligned(t, kc), kc)]

    def decay_rows(rows):
        low = dot(tokg[0, rows], lower[0:Co])
        for f in range(1, F):
            low += dot(tokg[f, rows], lower[f * Co : (f + 1) * Co])
        gate = dot(low.astype(BF16), local_up) + local_bias
        logsig = jnp.minimum(gate, 0.0) - jnp.log1p(jnp.exp(-jnp.abs(gate)))
        decay[rows, :] = logsig / TAU + extra[rows, :]

    loop(R, BAND, decay_rows)

    for i in range(1, F):
        owner = lax.rem(z + i, F)
        for s in range(S):
            arrived(piece(owner, s, 1 - g), qy_r.at[owner, s])

    def qkv_columns(cols):
        total = dot(tokg[0], wqkv[0, :, cols])
        for f in range(1, F):
            total += dot(tokg[f], wqkv[f, :, cols])
        qkv[:, cols] = total.astype(BF16)

    loop(W, TILE, qkv_columns)

    chunks = R // CHUNK
    scan_heads(
        heads, qkv, decay, head_gain[...], mixed,
        [(min(chunks - 1, 1 + 2 * i), out_event(i))
         for i in range(1, F)],
    )

    for i in range(1, F):
        owner = lax.rem(z + i, F)
        arrived(out_piece(owner, 1 - g), oy_r.at[owner])
    for i in range(X):
        j = lax.rem(x + 1 + i, X)
        for u in range(U):
            k, block = i * U + u, (2 * j + 1 - c) * U + u

            def other_rows(rows, k=k, block=block):
                mp[k, rows] = dot(mixed[rows], wout[block]).astype(BF16)

            loop(R, TILE, other_rows)
            sends.start(mp.at[k], md.at[k], md_s.at[k], md_r.at[k], at_core)
    for i in range(X):
        j = lax.rem(x + 1 + i, X)
        for u in range(U):
            k, block = i * U + u, (2 * j + c) * U + u
            arrived(md.at[k], md_r.at[k])

            def own_rows(rows, i=i, u=u, k=k, block=block):
                total = dot(mixed[rows], wout[block]) + md[k, rows].astype(F32)
                if i < X - 1:
                    xs[k, rows] = total.astype(BF16)
                else:
                    mk[u, rows] = total

            loop(R, TILE, own_rows)
            if i < X - 1:
                sends.start(xs.at[k], xr.at[x, u], mx_s.at[k], mx_r.at[x, u], at_t(2 * j + c))
    for i in range(1, F):
        for s in range(S2):
            up_event(i, s)

    def share_stats(slot):
        mine = st.at[slot]
        for i in range(1, T):
            to = lax.rem(t + i, T)
            sends.start(mine, sta.at[slot, t], st_s.at[slot, to], st_r.at[slot, t], at_t(to))

    def row_stats(slot, rows, parts):
        ones = jnp.ones((8, Co), F32)
        for kind in range(2):
            total = None
            for part in parts:
                term = lax.dot_general(
                    ones, part * part if kind else part, NT,
                    precision=lax.Precision.HIGHEST, preferred_element_type=F32,
                )
                total = term if total is None else total + term
            st[slot, kind, :, rows] = total
            sta[slot, t, kind, :, rows] = total

    def await_stats(slot):
        for i in range(1, T):
            owner = lax.rem(t + i, T)
            arrived(sta.at[slot, owner], st_r.at[slot, owner])

    def scale_of(slot, rows):
        totals = []
        for kind in range(2):
            total = sta[slot, 0, kind, :, rows]
            for other in range(1, T):
                total += sta[slot, other, kind, :, rows]
            totals.append(total / (Co * F))
        mean = totals[0]
        scale = lax.rsqrt(totals[1] - mean * mean + EPS)
        return mean.T[:, 0:1], scale.T[:, 0:1]

    for i in range(1, X):
        j = lax.rem(x + i, X)
        for u in range(U):
            arrived(xr.at[j, u], mx_r.at[j, u])

    def mix_rows(rows):
        parts = []
        for u in range(U):
            total = mk[u, rows]
            for i in range(1, X):
                total += xr[lax.rem(x + i, X), u, rows].astype(F32)
            total += ALPHA * tokg[t * U + u, rows].astype(F32)
            v[u, rows] = total
            parts.append(total)
        row_stats(0, rows, parts)

    loop(R, BAND, mix_rows)
    share_stats(0)
    await_stats(0)

    def norm_rows(rows):
        mean, scale = scale_of(0, rows)
        for u in range(U):
            gain = mix_gain[:, u * Co : (u + 1) * Co]
            normg[h, t * U + u, rows] = ((v[u, rows] - mean) * scale * gain).astype(BF16)

    loop(R, BAND, norm_rows)

    def region(pair, owner):
        return normg.at[pair, pl.ds(owner * U, U)]

    def forward(pair, owner, slot, device):
        mine = region(pair, owner)
        sends.start(mine, mine, nm_s.at[pair, owner, slot], nm_r.at[pair, owner], device)

    def await_region(pair, owner):
        arrived(region(pair, owner), nm_r.at[pair, owner])

    forward(h, t, X, at_z(mate))
    for i in range(1, X):
        forward(h, t, i, at_t(2 * lax.rem(x + i, X) + c))
    forward(h, t, 0, at_core)
    for i in range(1, X):
        owner = 2 * lax.rem(x + i, X) + c
        await_region(h, owner)
        forward(h, owner, 0, at_core)
    await_region(1 - h, t)
    for i in range(1, X):
        forward(1 - h, t, i, at_t(2 * lax.rem(x + i, X) + c))
    forward(1 - h, t, 0, at_core)
    for i in range(1, F):
        owner = lax.rem(z + i, F)
        for s in range(S2):
            arrived(up_piece(owner, s, 1 - g), uy_r.at[owner, s])

    def hidden(pair):
        for i in range(X):
            await_region(pair, 2 * lax.rem(x + i, X) + 1 - c)

        def hidden_columns(cols):
            total = dot(normg[pair, 0], wup[0, :, cols])
            for f in range(1, F):
                total += dot(normg[pair, f], wup[f, :, cols])
            act[pair, :, cols] = jnp.square(jnp.maximum(total, 0.0)).astype(BF16)

        loop(FH, TILE, hidden_columns)

    hidden(h)
    for i in range(1, X):
        owner = 2 * lax.rem(x + i, X) + c
        await_region(1 - h, owner)
        forward(1 - h, owner, 0, at_core)
    hidden(1 - h)

    for i in range(1, F):
        for s in range(S2):
            down_event(i, s)
    for i in range(1, F):
        owner = lax.rem(z + i, F)
        for s in range(S2):
            arrived(down_piece(owner, s, 1 - g), dy_r.at[owner, s])
    for i in range(X):
        j = lax.rem(x + 1 + i, X)
        for u in range(U):
            k, block = i * U + u, (2 * j + 1 - c) * U + u
            for slot, pair in enumerate((1 - h, h)):

                def other_rows(rows, k=k, block=block, slot=slot, pair=pair):
                    dnp[k, slot, rows] = dot(act[pair, rows], wdown[block]).astype(BF16)

                loop(R, TILE, other_rows)
                sends.start(
                    dnp.at[k, slot], dnd.at[k, slot], dd_s.at[k, slot], dd_r.at[k, slot], at_core
                )
    for i in range(X):
        j = lax.rem(x + 1 + i, X)
        for u in range(U):
            k, block = i * U + u, (2 * j + c) * U + u
            for slot, pair in enumerate((1 - h, h)):
                arrived(dnd.at[k, slot], dd_r.at[k, slot])

                def own_rows(rows, k=k, block=block, slot=slot, pair=pair):
                    total = dot(act[pair, rows], wdown[block]) + dnd[k, slot, rows].astype(F32)
                    if slot == 0:
                        dzs[k, rows] = total.astype(BF16)
                    else:
                        ck[k, rows] = total

                loop(R, TILE, own_rows)
                if slot == 0:
                    sends.start(dzs.at[k], dzr.at[k], dp_s.at[k], dp_r.at[k], at_z(mate))
    for i in range(X):
        j = lax.rem(x + 1 + i, X)
        for u in range(U):
            k = i * U + u
            arrived(dzr.at[k], dp_r.at[k])
            if i < X - 1:

                def pair_rows(rows, k=k):
                    dxs[k, rows] = (ck[k, rows] + dzr[k, rows].astype(F32)).astype(BF16)

                loop(R, BAND, pair_rows)
                sends.start(dxs.at[k], dxr.at[x, u], dx_s.at[k], dx_r.at[x, u], at_t(2 * j + c))
    for i in range(1, X):
        j = lax.rem(x + i, X)
        for u in range(U):
            arrived(dxr.at[j, u], dx_r.at[j, u])

    def last_rows(rows):
        parts = []
        for u in range(U):
            k = (X - 1) * U + u
            total = ck[k, rows] + dzr[k, rows].astype(F32)
            for i in range(1, X):
                total += dxr[lax.rem(x + i, X), u, rows].astype(F32)
            total += ALPHA * normg[h, t * U + u, rows].astype(F32)
            v[u, rows] = total
            parts.append(total)
        row_stats(1, rows, parts)

    loop(R, BAND, last_rows)
    share_stats(1)
    await_stats(1)

    def result_rows(rows):
        mean, scale = scale_of(1, rows)
        for u in range(U):
            gain = out_gain[:, u * Co : (u + 1) * Co]
            result[rows, u * Co : (u + 1) * Co] = ((v[u, rows] - mean) * scale * gain).astype(BF16)

    loop(R, BAND, result_rows)
    sends.drain()


def local(F, T, *args):
    (tokens, query, key, value, lower, decay_up, decay_bias, extra, head_gain, out_weight,
     mix_gain, up, down, out_gain) = args
    U, X = F // T, T // 2
    R, Dt = tokens.shape
    Co = Dt // U
    Rz, kc = query.shape
    W = 2 * kc + value.shape[1]
    Ko = out_weight.shape[0]
    FH = up.shape[1] // 2
    heads = kc // DK
    S, S2 = 2, 2
    vmem, hbm = pl.BlockSpec(memory_space=pltpu.VMEM), pl.BlockSpec(memory_space=pl.ANY)
    sem = lambda *shape: pltpu.SemaphoreType.DMA(shape)
    buf = lambda *shape: pltpu.VMEM(shape, BF16)
    wide = lambda *shape: pltpu.VMEM(shape, F32)
    H = X * U
    scratch = [
        buf(F, R, Co), buf(F, Rz, W), buf(F, Ko, Co), buf(F, Rz, FH), buf(F, FH, Co),
        buf(R, W), wide(R, kc), buf(R, heads * DV),
        buf(H, R, Co), buf(H, R, Co), buf(H, R, Co), buf(X, U, R, Co), wide(U, R, Co),
        wide(U, R, Co), wide(2, 2, 8, R), wide(2, T, 2, 8, R), buf(2, F, R, Co), buf(2, R, FH),
        buf(H, 2, R, Co), buf(H, 2, R, Co), wide(H, R, Co), buf(H, R, Co), buf(H, R, Co),
        buf(H, R, Co), buf(X, U, R, Co),
        sem(6 + U), sem(T), sem(T), sem(2, F, S), sem(F, S), sem(F, S), sem(F, S),
        sem(F), sem(F), sem(F), sem(F),
        sem(F, S2), sem(F, S2), sem(F, S2), sem(F, S2),
        sem(F, S2), sem(F, S2), sem(F, S2), sem(F, S2),
        sem(H), sem(H), sem(H), sem(X, U), sem(2, T), sem(2, T), sem(2, T, X + 1), sem(2, T),
        sem(H, 2), sem(H, 2), sem(H), sem(H), sem(H), sem(X, U),
    ]
    return pl.pallas_call(
        functools.partial(kernel, F, T),
        out_shape=jax.ShapeDtypeStruct((R, Dt), BF16),
        in_specs=[hbm, hbm, hbm, hbm, vmem, vmem, vmem, vmem, vmem, hbm, vmem, hbm, hbm, vmem],
        out_specs=vmem,
        scratch_shapes=scratch,
        compiler_params=pltpu.CompilerParams(
            collective_id=0, has_side_effects=True, vmem_limit_bytes=63 * 2**20
        ),
        name="layer",
    )(
        tokens, query, key, value, lower, decay_up, decay_bias[None], extra, head_gain[None],
        out_weight, mix_gain[None], up, down, out_gain[None],
    )


def solution(mesh):
    in_specs = (
        P(("grp", "fs"), "tp"),
        P("fs", "tp"),
        P("fs", "tp"),
        P("fs", "tp"),
        P(),
        P(),
        P(),
        P(("grp", "fs"), "tp"),
        P(),
        P("tp", "fs"),
        P("tp"),
        P("fs", "tp"),
        P("tp", "fs"),
        P("tp"),
    )
    out_specs = P(("grp", "fs"), "tp")
    body = functools.partial(local, mesh.shape["fs"], mesh.shape["tp"])
    return jax.shard_map(body, mesh=mesh, in_specs=in_specs, out_specs=out_specs, check_vma=False)
```

```python
import functools

import jax
import jax.numpy as jnp
from jax import lax
from jax.experimental import pallas as pl
from jax.experimental.pallas import tpu as pltpu
from jax.sharding import PartitionSpec as P

DK = 128
DV = 256
CHUNK = 64
SUB = 16
TILE = 256
BAND = 128

ALPHA = 2.0**0.5
TAU = 16.0
EPS = 1e-05

MESH = pl.DeviceIdType.MESH
NT = (((1,), (1,)), ((), ()))
TN = (((0,), (0,)), ((), ()))
BF16, F32 = jnp.bfloat16, jnp.float32


def dot(a, b):
    return jnp.dot(a, b, preferred_element_type=F32)


def loop(count, size, body):
    def step(index, carry):
        body(pl.ds(pl.multiple_of(index * size, size), size))
        return carry

    lax.fori_loop(0, count // size, step, 0)


def when(cond, body):
    if cond is None:
        body()
    else:
        pl.when(cond)(body)


class Sends:
    def __init__(self):
        self.open = []

    def start(self, src, dst, send, recv, device, cond=None):
        def copy():
            return pltpu.make_async_remote_copy(
                src_ref=src, dst_ref=dst, send_sem=send, recv_sem=recv,
                device_id=device, device_id_type=MESH,
            )

        when(cond, lambda: copy().start())
        self.open.append((cond, copy))

    def drain(self):
        for cond, copy in self.open:
            when(cond, lambda copy=copy: copy().wait_send())
        self.open = []


def scan_heads(heads, qkv_ref, decay_ref, gain, out_ref, events):
    rows = qkv_ref.shape[0]
    at_row = lax.broadcasted_iota(jnp.int32, (CHUNK, CHUNK), 0)
    at_col = lax.broadcasted_iota(jnp.int32, (CHUNK, CHUNK), 1)
    tri = (at_row >= at_col).astype(F32)
    sub_row = lax.broadcasted_iota(jnp.int32, (SUB, SUB), 0)
    sub_col = lax.broadcasted_iota(jnp.int32, (SUB, SUB), 1)

    def step(index, states):
        for at, event in events:
            pl.when(index == at)(event)
        here = pl.ds(pl.multiple_of(index * CHUNK, CHUNK), CHUNK)
        fresh_states = []
        for head in range(heads):
            query = qkv_ref[here, head * DK : (head + 1) * DK].astype(F32) * DK**-0.5
            keys = qkv_ref[here, (heads + head) * DK : (heads + head + 1) * DK].astype(F32)
            at_value = 2 * heads * DK + head * DV
            value = qkv_ref[here, at_value : at_value + DV]
            decay = decay_ref[here, head * DK : (head + 1) * DK]
            cumul = jnp.dot(
                tri, decay, precision=lax.Precision.HIGHEST, preferred_element_type=F32
            )
            last = cumul[CHUNK - 1 : CHUNK, :]
            state = states[head]
            out = lax.dot_general(
                (query * jnp.exp(cumul)).astype(BF16),
                state.astype(BF16),
                NT,
                preferred_element_type=F32,
            )
            strips = []
            for a in range(CHUNK // SUB):
                lo, hi = a * SUB, (a + 1) * SUB
                q_a, k_a, g_a = query[lo:hi], keys[lo:hi], cumul[lo:hi]
                diag = jnp.zeros((SUB, SUB), F32)
                for j in range(SUB):
                    weight = jnp.exp(jnp.minimum(g_a - g_a[j : j + 1], 0.0))
                    column = jnp.sum(q_a * k_a[j : j + 1] * weight, axis=1, keepdims=True)
                    diag = jnp.where((sub_col == j) & (sub_row >= j), column, diag)
                strip = dot(diag.astype(BF16), value[lo:hi])
                if a:
                    base = cumul[lo - 1 : lo]
                    before = lax.dot_general(
                        (q_a * jnp.exp(g_a - base)).astype(BF16),
                        (keys[:lo] * jnp.exp(base - cumul[:lo])).astype(BF16),
                        NT,
                        preferred_element_type=F32,
                    )
                    strip += dot(before.astype(BF16), value[:lo])
                strips.append(strip)
            out = out + jnp.concatenate(strips, axis=0)
            fresh = lax.dot_general(
                value,
                (keys * jnp.exp(last - cumul)).astype(BF16),
                TN,
                preferred_element_type=F32,
            )
            fresh_states.append(state * jnp.exp(last) + fresh)
            mean = jnp.mean(out * out, axis=1, keepdims=True)
            out_ref[here, head * DV : (head + 1) * DV] = (
                out * lax.rsqrt(mean + EPS) * gain
            ).astype(BF16)
        return tuple(fresh_states)

    start = tuple(jnp.zeros((DV, DK), F32) for _ in range(heads))
    lax.fori_loop(0, rows // CHUNK, step, start)


def kernel(
    F, T,
    tokens, query, key, value, lower, decay_up, decay_bias, extra, head_gain, out_weight,
    mix_gain, up, down, out_gain,
    result,
    tokg, wqkv, wout, wup, wdown, qkv, decay, mixed, mp, md, xs, xr, mk, v, st, sta, normg, act,
    dnp, dnd, ck, dzs, dzr, dxs, dxr,
    loc, tok_s, tok_r, qz_s, qz_r, qy_s, qy_r, oz_s, oz_r, oy_s, oy_r, uz_s, uz_r, uy_s, uy_r,
    dz_s, dz_r, dy_s, dy_r, md_s, md_r, mx_s, mx_r, st_s, st_r, nm_s, nm_r, dd_s, dd_r,
    dp_s, dp_r, dx_s, dx_r,
):
    U, X = F // T, T // 2
    R, Co = v.shape[1], v.shape[2]
    Rz, W = wqkv.shape[1], wqkv.shape[2]
    kc, vc = query.shape[1], value.shape[1]
    Ko, FH = wout.shape[1], wup.shape[2]
    S = qz_s.shape[2]
    S2, S3 = uz_s.shape[1], dz_s.shape[1]
    heads = kc // DK
    g, z, t = lax.axis_index("grp"), lax.axis_index("fs"), lax.axis_index("tp")
    x, c = lax.div(t, 2), lax.rem(t, 2)
    h = lax.rem(z, 2)
    mate = z + 1 - 2 * h
    sends = Sends()

    at_z = lambda other: (g, other, t)
    at_t = lambda other: (g, z, other)
    at_y = (1 - g, z, t)
    at_core = (g, z, t + 1 - 2 * c)
    core = t + 1 - 2 * c

    def arrived(dst, sem, cond=None):
        when(cond, lambda: pltpu.make_async_remote_copy(
            src_ref=dst, dst_ref=dst, send_sem=sem, recv_sem=sem,
            device_id=at_y, device_id_type=MESH,
        ).wait_recv())

    def aligned(value, size):
        return pl.multiple_of(value * size, size)

    copies = [
        pltpu.make_async_copy(query, wqkv.at[z, :, pl.ds(0, kc)], loc.at[0]),
        pltpu.make_async_copy(key, wqkv.at[z, :, pl.ds(kc, kc)], loc.at[1]),
        pltpu.make_async_copy(value, wqkv.at[z, :, pl.ds(2 * kc, vc)], loc.at[2]),
    ]
    tok_copies = [
        pltpu.make_async_copy(tokens.at[:, pl.ds(u * Co, Co)], tokg.at[t * U + u], loc.at[3 + u])
        for u in range(U)
    ]
    late_copies = [
        pltpu.make_async_copy(out_weight, wout.at[z], loc.at[3 + U]),
        pltpu.make_async_copy(up.at[:, pl.ds(aligned(h, FH), FH)], wup.at[z], loc.at[4 + U]),
        pltpu.make_async_copy(down.at[pl.ds(aligned(h, FH), FH), :], wdown.at[z], loc.at[5 + U]),
    ]
    for copy in copies + tok_copies + late_copies:
        copy.start()

    barrier = pltpu.get_barrier_semaphore()
    partners = [at_y]
    partners += [at_z(lax.rem(z + i, F)) for i in range(1, F)]
    partners += [at_t(lax.rem(t + i, T)) for i in range(1, T)]
    for device in partners:
        pl.semaphore_signal(barrier, inc=1, device_id=device, device_id_type=MESH)
    pl.semaphore_wait(barrier, len(partners))

    half = Rz // 2
    step = half // S

    def piece(owner, s, side):
        return wqkv.at[owner, pl.ds(pl.multiple_of(side * half + s * step, step), step), :]

    for copy in copies:
        copy.wait()
    for s in range(S):
        for way, cond in ((0, z < F - 1), (1, z > 0)):
            to = z + 1 - 2 * way
            sends.start(piece(z, s, g), piece(z, s, g), qz_s.at[way, z, s], qz_r.at[z, s], at_z(to), cond)
    for copy in tok_copies:
        copy.wait()
    for i in range(1, T):
        to = lax.rem(t + i, T)
        mine = tokg.at[pl.ds(t * U, U)]
        sends.start(mine, mine, tok_s.at[to], tok_r.at[t], at_t(to))
    def out_piece(owner, side):
        return wout.at[owner, pl.ds(aligned(side, Ko // 2), Ko // 2), :]

    def up_piece(owner, s, side):
        size = Rz // 2 // S2
        return wup.at[owner, pl.ds(pl.multiple_of(side * (Rz // 2) + s * size, size), size), :]

    def columns(s):
        return pl.ds(s * (Co // S3), Co // S3)

    def down_piece(owner, s, side):
        return wdown.at[owner, pl.ds(aligned(side, FH // 2), FH // 2), columns(s)]

    def others(d):
        return ((z + d, z + d < F), (z - d, z >= d))

    def send_up(d, s, ways=(None, None)):
        size = Rz // 2 // S2
        rows = pl.ds(pl.multiple_of(g * (Rz // 2) + s * size, size), size)
        part = lax.rem(h + d, 2)
        for (to, there), way in zip(others(d), ways):
            there = there if way is None else there & way
            sends.start(
                up.at[rows, pl.ds(aligned(part, FH), FH)], up_piece(z, s, g),
                uz_s.at[to, s], uz_r.at[z, s], at_z(to), there,
            )

    def send_down(d, s, ways=(None, None)):
        part = lax.rem(h + d, 2)
        rows = pl.ds(aligned(2 * part + g, FH // 2), FH // 2)
        for (to, there), way in zip(others(d), ways):
            there = there if way is None else there & way
            sends.start(
                down.at[rows, columns(s)], down_piece(z, s, g), dz_s.at[to, s], dz_r.at[z, s], at_z(to),
                there,
            )

    def stream(d, mine_of, send, recv, y_send, y_recv, inner_only):
        for way, (owner, there) in enumerate(((z - d, z >= d), (z + d, z + d < F))):
            onward = there & ((z < F - 1) if way == 0 else (z > 0))
            if inner_only:
                there = onward
            mine, here = mine_of(owner), recv(owner)
            arrived(mine, here, there)
            sends.start(mine, mine, send(way, owner), here, at_z(z + 1 - 2 * way), onward)
            sends.start(mine, mine, y_send(owner), y_recv(owner), at_y, there)

    def stream_late(d):
        steps = []
        for way, (owner, there) in enumerate(((z - d, z >= d), (z + d, z + d < F))):
            inner = (z < F - 1) if way == 0 else (z > 0)
            ends = (z == F - 1) if way == 0 else (z == 0)
            onward = there & inner
            if d <= F // 2:
                there, onward = there & ends, None
            steps.append((
                out_piece(owner, g), oz_r.at[owner], there, onward, oz_s.at[way, owner],
                at_z(z + 1 - 2 * way), oy_s.at[owner], oy_r.at[owner],
            ))

        def event():
            for mine, here, there, onward, send, to, y_send, y_recv in steps:
                arrived(mine, here, there)
                if onward is not None:
                    sends.start(mine, mine, send, here, to, onward)
                sends.start(mine, mine, y_send, y_recv, at_y, there)

        return event

    def stream_qkv(d, s):
        stream(
            d, lambda o: piece(o, s, g), lambda w, o: qz_s.at[w, o, s], lambda o: qz_r.at[o, s],
            lambda o: qy_s.at[o, s], lambda o: qy_r.at[o, s], False,
        )

    def stream_out(d):
        stream(
            d, lambda o: out_piece(o, g), lambda w, o: oz_s.at[w, o], lambda o: oz_r.at[o],
            lambda o: oy_s.at[o], lambda o: oy_r.at[o], True,
        )

    for d in range(1, F):
        for s in range(S):
            stream_qkv(d, s)
        if d == F // 2:
            late_copies[0].wait()
            for way, cond in ((0, z < F - 1), (1, z > 0)):
                mine = out_piece(z, g)
                sends.start(mine, mine, oz_s.at[way, z], oz_r.at[z], at_z(z + 1 - 2 * way), cond)
    for d in range(1, F // 2 + 1):
        stream_out(d)
    even, odd = h == 0, h == 1
    for s in range(S2):
        send_up(1, s)
        send_up(2, s, (even, odd))
    for copy in late_copies[1:]:
        copy.wait()

    def swaps(d, make, z_sem, y_send, y_recv, ways=(None, None)):
        events = []
        for (owner, there), way in zip(others(d), ways):
            there = there if way is None else there & way
            mine, near, send, recv = make(owner), z_sem(owner), y_send(owner), y_recv(owner)

            def event(mine=mine, near=near, send=send, recv=recv, there=there):
                arrived(mine, near, there)
                sends.start(mine, mine, send, recv, at_y, there)

            events.append(event)
        def run():
            for event in events:
                event()

        return run

    def up_swap(d, s):
        return swaps(
            d, lambda o: up_piece(o, s, g), lambda o: uz_r.at[o, s], lambda o: uy_s.at[o, s],
            lambda o: uy_r.at[o, s],
        )

    def down_swap(d, s, ways=(None, None)):
        return swaps(
            d, lambda o: down_piece(o, s, g), lambda o: dz_r.at[o, s], lambda o: dy_s.at[o, s],
            lambda o: dy_r.at[o, s], ways,
        )

    for i in range(1, T):
        owner = lax.rem(t + i, T)
        arrived(tokg.at[pl.ds(owner * U, U)], tok_r.at[owner])
    local_up = decay_up[:, pl.ds(aligned(t, kc), kc)]
    local_bias = decay_bias[:, pl.ds(aligned(t, kc), kc)]

    def decay_rows(rows):
        low = jnp.zeros((BAND, lower.shape[0]), F32)
        for f in range(F):
            low += lax.dot_general(
                tokg[f, rows], lower[:, f * Co : (f + 1) * Co], NT, preferred_element_type=F32
            )
        gate = dot(low.astype(BF16), local_up) + local_bias
        logsig = jnp.minimum(gate, 0.0) - jnp.log1p(jnp.exp(-jnp.abs(gate)))
        decay[rows, :] = logsig / TAU + extra[rows, :]

    loop(R, BAND, decay_rows)

    for i in range(1, F):
        owner = lax.rem(z + i, F)
        for s in range(S):
            arrived(piece(owner, s, 1 - g), qy_r.at[owner, s])

    def qkv_columns(cols):
        total = dot(tokg[0], wqkv[0, :, cols])
        for f in range(1, F):
            total += dot(tokg[f], wqkv[f, :, cols])
        qkv[:, cols] = total.astype(BF16)

    loop(W, TILE, qkv_columns)

    chunks = R // CHUNK
    events = []
    for d in range(1, F):
        events.append((min(chunks - 1, 2 * d - 1), stream_late(d)))
    scan_heads(heads, qkv, decay, head_gain[...], mixed, events)

    for s in range(S2):
        send_up(2, s, (odd, even))
        for d in range(3, F):
            send_up(d, s)
    for s in range(S3):
        send_down(1, s, (odd, even))
    for i in range(1, F):
        owner = lax.rem(z + i, F)
        arrived(out_piece(owner, 1 - g), oy_r.at[owner])
    for i in range(X):
        j = lax.rem(x + 1 + i, X)
        for u in range(U):
            k, block = i * U + u, (2 * j + 1 - c) * U + u

            def other_rows(rows, k=k, block=block):
                mp[k, rows] = dot(mixed[rows], wout[block]).astype(BF16)

            loop(R, TILE, other_rows)
            sends.start(mp.at[k], md.at[k], md_s.at[k], md_r.at[k], at_core)
    for i in range(X):
        j = lax.rem(x + 1 + i, X)
        for u in range(U):
            k, block = i * U + u, (2 * j + c) * U + u
            arrived(md.at[k], md_r.at[k])

            def own_rows(rows, i=i, u=u, k=k, block=block):
                total = dot(mixed[rows], wout[block]) + md[k, rows].astype(F32)
                if i < X - 1:
                    xs[k, rows] = total.astype(BF16)
                else:
                    mk[u, rows] = total

            loop(R, TILE, own_rows)
            if i < X - 1:
                sends.start(xs.at[k], xr.at[x, u], mx_s.at[k], mx_r.at[x, u], at_t(2 * j + c))
    up_swap(1, 0)()

    def share_stats(slot):
        mine = st.at[slot]
        for i in range(1, T):
            to = lax.rem(t + i, T)
            sends.start(mine, sta.at[slot, t], st_s.at[slot, to], st_r.at[slot, t], at_t(to))

    def row_stats(slot, rows, parts):
        ones = jnp.ones((8, Co), F32)
        for kind in range(2):
            total = None
            for part in parts:
                term = lax.dot_general(
                    ones, part * part if kind else part, NT,
                    precision=lax.Precision.HIGHEST, preferred_element_type=F32,
                )
                total = term if total is None else total + term
            st[slot, kind, :, rows] = total
            sta[slot, t, kind, :, rows] = total

    def await_stats(slot):
        for i in range(1, T):
            owner = lax.rem(t + i, T)
            arrived(sta.at[slot, owner], st_r.at[slot, owner])

    def scale_of(slot, rows):
        totals = []
        for kind in range(2):
            total = sta[slot, 0, kind, :, rows]
            for other in range(1, T):
                total += sta[slot, other, kind, :, rows]
            totals.append(total / (Co * F))
        mean = totals[0]
        scale = lax.rsqrt(totals[1] - mean * mean + EPS)
        return mean.T[:, 0:1], scale.T[:, 0:1]

    for i in range(1, X):
        j = lax.rem(x + i, X)
        for u in range(U):
            arrived(xr.at[j, u], mx_r.at[j, u])

    def mix_rows(rows):
        parts = []
        for u in range(U):
            total = mk[u, rows]
            for i in range(1, X):
                total += xr[lax.rem(x + i, X), u, rows].astype(F32)
            total += ALPHA * tokg[t * U + u, rows].astype(F32)
            v[u, rows] = total
            parts.append(total)
        row_stats(0, rows, parts)

    loop(R, BAND, mix_rows)
    share_stats(0)
    await_stats(0)

    def norm_rows(rows):
        mean, scale = scale_of(0, rows)
        for u in range(U):
            gain = mix_gain[:, u * Co : (u + 1) * Co]
            normg[h, t * U + u, rows] = ((v[u, rows] - mean) * scale * gain).astype(BF16)

    loop(R, BAND, norm_rows)

    def region(pair, owner):
        return normg.at[pair, pl.ds(owner * U, U)]

    def forward(pair, owner, slot, device):
        mine = region(pair, owner)
        sends.start(mine, mine, nm_s.at[pair, owner, slot], nm_r.at[pair, owner], device)

    def await_region(pair, owner):
        arrived(region(pair, owner), nm_r.at[pair, owner])

    forward(h, t, X, at_z(mate))
    for i in range(1, X):
        forward(h, t, i, at_t(2 * lax.rem(x + i, X) + c))
    forward(h, t, 0, at_core)
    for s in range(S3):
        send_down(1, s, (even, odd))
        send_down(2, s, (even, odd))
    for s in range(1, S2):
        up_swap(1, s)()
    for s in range(S2):
        for d in range(2, F):
            up_swap(d, s)()
    await_region(1 - h, t)
    for s in range(S3):
        send_down(2, s, (odd, even))
        for d in range(3, F):
            send_down(d, s)
    for i in range(1, X):
        forward(1 - h, t, i, at_t(2 * lax.rem(x + i, X) + c))
    forward(1 - h, t, 0, at_core)
    ends = (z == 0) | (z == F - 1)
    inside = (z > 0) & (z < F - 1)
    for s in range(S3):
        down_swap(1, s, (odd, even))()
        down_swap(1, s, (even & ends, odd & ends))()
    for i in range(1, X):
        owner = 2 * lax.rem(x + i, X) + c
        await_region(h, owner)
        forward(h, owner, 0, at_core)
    for i in range(1, F):
        owner = lax.rem(z + i, F)
        for s in range(S2):
            arrived(up_piece(owner, s, 1 - g), uy_r.at[owner, s])

    def hidden(pair):
        for i in range(X):
            await_region(pair, 2 * lax.rem(x + i, X) + 1 - c)

        def hidden_columns(cols):
            total = dot(normg[pair, 0], wup[0, :, cols])
            for f in range(1, F):
                total += dot(normg[pair, f], wup[f, :, cols])
            act[pair, :, cols] = jnp.square(jnp.maximum(total, 0.0)).astype(BF16)

        loop(FH, TILE, hidden_columns)

    hidden(h)
    for s in range(S3):
        down_swap(1, s, (even & inside, odd & inside))()
    for i in range(1, X):
        owner = 2 * lax.rem(x + i, X) + c
        await_region(1 - h, owner)
        forward(1 - h, owner, 0, at_core)
    late = [(d, s) for s in range(S3) for d in range(2, F)]
    hidden(1 - h)

    pair_of = lax.div(z, 2)
    bands = [pl.ds(r * BAND, BAND) for r in range(R // BAND)]

    def await_down(block, s):
        arrived(down_piece(block, s, 1 - g), dy_r.at[block, s], block != z)

    def project(i, j, u, s):
        k, cols = i * U + u, columns(s)
        block = (2 * j + 1 - c) * U + u
        for slot, pair in enumerate((1 - h, h)):

            def other_rows(rows, block=block, slot=slot, pair=pair):
                dnp[k, slot, rows, cols] = dot(act[pair, rows], wdown[block, :, cols]).astype(BF16)

            loop(R, TILE, other_rows)
            mine = (k, slot, slice(None), cols)
            sends.start(
                dnp.at[mine], dnd.at[mine], dd_s.at[k, slot, s], dd_r.at[k, slot, s], at_core
            )
        block = (2 * j + c) * U + u
        arrived(dnd.at[k, 0, :, cols], dd_r.at[k, 0, s])
        for r, rows in enumerate(bands):
            total = dot(act[1 - h, rows], wdown[block, :, cols])
            dzs[k, rows, cols] = (total + dnd[k, 0, rows, cols].astype(F32)).astype(BF16)
            sends.start(
                dzs.at[k, rows, cols], dzr.at[k, rows, cols], dp_s.at[k, r, s], dp_r.at[k, r, s],
                at_z(mate),
            )
        arrived(dnd.at[k, 1, :, cols], dd_r.at[k, 1, s])

        def own_rows(rows, block=block):
            total = dot(act[h, rows], wdown[block, :, cols])
            ck[k, rows, cols] = total + dnd[k, 1, rows, cols].astype(F32)

        loop(R, TILE, own_rows)

    def add_pair(i, j, u, s):
        k, cols = i * U + u, columns(s)
        for r, rows in enumerate(bands):
            arrived(dzr.at[k, rows, cols], dp_r.at[k, r, s])
            total = ck[k, rows, cols] + dzr[k, rows, cols].astype(F32)
            dxs[k, rows, cols] = total.astype(BF16)
            sends.start(
                dxs.at[k, rows, cols], dxr.at[x, u, rows, cols], dx_s.at[k, r, s],
                dx_r.at[x, u, r, s], at_t(2 * j + c), j != x,
            )

    if U > 1:
        for s in range(S3):
            for d in range(2, F):
                down_swap(d, s)()
    for i in range(X):
        j = lax.rem(pair_of + i, X)
        for s in range(S3):
            for block in range(2 * U):
                await_down(2 * j * U + block, s)
            for u in range(U):
                project(i, j, u, s)
            if i == 0 and U == 1:
                for d in range(2, F):
                    down_swap(d, s)()
        for s in range(S3):
            for u in range(U):
                add_pair(i, j, u, s)
    for i in range(1, X):
        j = lax.rem(x + i, X)
        for u in range(U):
            for s in range(S3):
                for r, rows in enumerate(bands):
                    arrived(dxr.at[j, u, rows, columns(s)], dx_r.at[j, u, r, s])
    own = lax.rem(x - lax.rem(pair_of, X) + X, X) * U

    def last_rows(rows):
        parts = []
        for u in range(U):
            total = ck[own + u, rows] + dzr[own + u, rows].astype(F32)
            for i in range(1, X):
                total += dxr[lax.rem(x + i, X), u, rows].astype(F32)
            total += ALPHA * normg[h, t * U + u, rows].astype(F32)
            v[u, rows] = total
            parts.append(total)
        row_stats(1, rows, parts)

    loop(R, BAND, last_rows)
    share_stats(1)
    await_stats(1)

    def result_rows(rows):
        mean, scale = scale_of(1, rows)
        for u in range(U):
            gain = out_gain[:, u * Co : (u + 1) * Co]
            result[rows, u * Co : (u + 1) * Co] = ((v[u, rows] - mean) * scale * gain).astype(BF16)

    loop(R, BAND, result_rows)
    sends.drain()


def local(F, T, *args):
    (tokens, query, key, value, lower, decay_up, decay_bias, extra, head_gain, out_weight,
     mix_gain, up, down, out_gain) = args
    U, X = F // T, T // 2
    R, Dt = tokens.shape
    Co = Dt // U
    Rz, kc = query.shape
    W = 2 * kc + value.shape[1]
    Ko = out_weight.shape[0]
    FH = up.shape[1] // 2
    heads = kc // DK
    S, S2, S3 = 2, 2, 2 if Co % (2 * DK) == 0 else 1
    vmem, hbm = pl.BlockSpec(memory_space=pltpu.VMEM), pl.BlockSpec(memory_space=pl.ANY)
    sem = lambda *shape: pltpu.SemaphoreType.DMA(shape)
    buf = lambda *shape: pltpu.VMEM(shape, BF16)
    wide = lambda *shape: pltpu.VMEM(shape, F32)
    H = X * U
    scratch = [
        buf(F, R, Co), buf(F, Rz, W), buf(F, Ko, Co), buf(F, Rz, FH), buf(F, FH, Co),
        buf(R, W), wide(R, kc), buf(R, heads * DV),
        buf(H, R, Co), buf(H, R, Co), buf(H, R, Co), buf(X, U, R, Co), wide(U, R, Co),
        wide(U, R, Co), wide(2, 2, 8, R), wide(2, T, 2, 8, R), buf(2, F, R, Co), buf(2, R, FH),
        buf(H, 2, R, Co), buf(H, 2, R, Co), wide(H, R, Co), buf(H, R, Co), buf(H, R, Co),
        buf(H, R, Co), buf(X, U, R, Co),
        sem(6 + U), sem(T), sem(T), sem(2, F, S), sem(F, S), sem(F, S), sem(F, S),
        sem(2, F), sem(F), sem(F), sem(F),
        sem(F, S2), sem(F, S2), sem(F, S2), sem(F, S2),
        sem(F, S3), sem(F, S3), sem(F, S3), sem(F, S3),
        sem(H), sem(H), sem(H), sem(X, U), sem(2, T), sem(2, T), sem(2, T, X + 1), sem(2, T),
        sem(H, 2, S3), sem(H, 2, S3), sem(H, R // BAND, S3), sem(H, R // BAND, S3),
        sem(H, R // BAND, S3), sem(X, U, R // BAND, S3),
    ]
    return pl.pallas_call(
        functools.partial(kernel, F, T),
        out_shape=jax.ShapeDtypeStruct((R, Dt), BF16),
        in_specs=[hbm, hbm, hbm, hbm, vmem, vmem, vmem, vmem, vmem, hbm, vmem, hbm, hbm, vmem],
        out_specs=vmem,
        scratch_shapes=scratch,
        compiler_params=pltpu.CompilerParams(
            collective_id=0, has_side_effects=True, vmem_limit_bytes=63 * 2**20
        ),
        name="layer",
    )(
        tokens, query, key, value, lower.T, decay_up, decay_bias[None], extra, head_gain[None],
        out_weight, mix_gain[None], up, down, out_gain[None],
    )


def solution(mesh):
    in_specs = (
        P(("grp", "fs"), "tp"),
        P("fs", "tp"),
        P("fs", "tp"),
        P("fs", "tp"),
        P(),
        P(),
        P(),
        P(("grp", "fs"), "tp"),
        P(),
        P("tp", "fs"),
        P("tp"),
        P("fs", "tp"),
        P("tp", "fs"),
        P("tp"),
    )
    out_specs = P(("grp", "fs"), "tp")
    body = functools.partial(local, mesh.shape["fs"], mesh.shape["tp"])
    return jax.shard_map(body, mesh=mesh, in_specs=in_specs, out_specs=out_specs, check_vma=False)
```

```python
import functools

import jax
import jax.numpy as jnp
from jax import lax
from jax.experimental import pallas as pl
from jax.experimental.pallas import tpu as pltpu
from jax.sharding import PartitionSpec as P

DK = 128
DV = 256
CHUNK = 64
SUB = 16
TILE = 256
BAND = 128

ALPHA = 2.0**0.5
TAU = 16.0
EPS = 1e-05

MESH = pl.DeviceIdType.MESH
NT = (((1,), (1,)), ((), ()))
TN = (((0,), (0,)), ((), ()))
BF16, F32 = jnp.bfloat16, jnp.float32


def dot(a, b):
    return jnp.dot(a, b, preferred_element_type=F32)


def loop(count, size, body):
    def step(index, carry):
        body(pl.ds(pl.multiple_of(index * size, size), size))
        return carry

    lax.fori_loop(0, count // size, step, 0)


def when(cond, body):
    if cond is None:
        body()
    else:
        pl.when(cond)(body)


class Sends:
    def __init__(self):
        self.open = []

    def start(self, src, dst, send, recv, device, cond=None):
        def copy():
            return pltpu.make_async_remote_copy(
                src_ref=src, dst_ref=dst, send_sem=send, recv_sem=recv,
                device_id=device, device_id_type=MESH,
            )

        when(cond, lambda: copy().start())
        self.open.append((cond, copy))

    def drain(self):
        for cond, copy in self.open:
            when(cond, lambda copy=copy: copy().wait_send())
        self.open = []


def scan_heads(heads, qkv_ref, decay_ref, gain, out_ref, events):
    rows = qkv_ref.shape[0]
    at_row = lax.broadcasted_iota(jnp.int32, (CHUNK, CHUNK), 0)
    at_col = lax.broadcasted_iota(jnp.int32, (CHUNK, CHUNK), 1)
    tri = (at_row >= at_col).astype(F32)
    sub_row = lax.broadcasted_iota(jnp.int32, (SUB, SUB), 0)
    sub_col = lax.broadcasted_iota(jnp.int32, (SUB, SUB), 1)

    def step(index, states):
        for at, event in events:
            pl.when(index == at)(event)
        here = pl.ds(pl.multiple_of(index * CHUNK, CHUNK), CHUNK)
        fresh_states = []
        for head in range(heads):
            query = qkv_ref[here, head * DK : (head + 1) * DK].astype(F32) * DK**-0.5
            keys = qkv_ref[here, (heads + head) * DK : (heads + head + 1) * DK].astype(F32)
            at_value = 2 * heads * DK + head * DV
            value = qkv_ref[here, at_value : at_value + DV]
            decay = decay_ref[here, head * DK : (head + 1) * DK]
            cumul = jnp.dot(
                tri, decay, precision=lax.Precision.HIGHEST, preferred_element_type=F32
            )
            last = cumul[CHUNK - 1 : CHUNK, :]
            state = states[head]
            out = lax.dot_general(
                (query * jnp.exp(cumul)).astype(BF16),
                state.astype(BF16),
                NT,
                preferred_element_type=F32,
            )
            strips = []
            for a in range(CHUNK // SUB):
                lo, hi = a * SUB, (a + 1) * SUB
                q_a, k_a, g_a = query[lo:hi], keys[lo:hi], cumul[lo:hi]
                diag = jnp.zeros((SUB, SUB), F32)
                for j in range(SUB):
                    weight = jnp.exp(jnp.minimum(g_a - g_a[j : j + 1], 0.0))
                    column = jnp.sum(q_a * k_a[j : j + 1] * weight, axis=1, keepdims=True)
                    diag = jnp.where((sub_col == j) & (sub_row >= j), column, diag)
                strip = dot(diag.astype(BF16), value[lo:hi])
                if a:
                    base = cumul[lo - 1 : lo]
                    before = lax.dot_general(
                        (q_a * jnp.exp(g_a - base)).astype(BF16),
                        (keys[:lo] * jnp.exp(base - cumul[:lo])).astype(BF16),
                        NT,
                        preferred_element_type=F32,
                    )
                    strip += dot(before.astype(BF16), value[:lo])
                strips.append(strip)
            out = out + jnp.concatenate(strips, axis=0)
            fresh = lax.dot_general(
                value,
                (keys * jnp.exp(last - cumul)).astype(BF16),
                TN,
                preferred_element_type=F32,
            )
            fresh_states.append(state * jnp.exp(last) + fresh)
            mean = jnp.mean(out * out, axis=1, keepdims=True)
            out_ref[here, head * DV : (head + 1) * DV] = (
                out * lax.rsqrt(mean + EPS) * gain
            ).astype(BF16)
        return tuple(fresh_states)

    start = tuple(jnp.zeros((DV, DK), F32) for _ in range(heads))
    lax.fori_loop(0, rows // CHUNK, step, start)


def kernel(
    F, T,
    tokens, query, key, value, lower, decay_up, decay_bias, extra, head_gain, out_weight,
    mix_gain, up, down, out_gain,
    result,
    tokg, wqkv, wout, wup, wdown, qkv, decay, mixed, mp, md, xs, xr, mk, v, st, sta, normg, act,
    dnp, dnd, ck, dzs, dzr, dxs, dxr,
    loc, tok_s, tok_r, qz_s, qz_r, qy_s, qy_r, oz_s, oz_r, oy_s, oy_r, uz_s, uz_r, uy_s, uy_r,
    dz_s, dz_r, dy_s, dy_r, md_s, md_r, mx_s, mx_r, st_s, st_r, nm_s, nm_r, dd_s, dd_r,
    dp_s, dp_r, dx_s, dx_r,
):
    U, X = F // T, T // 2
    R, Co = v.shape[1], v.shape[2]
    Rz, W = wqkv.shape[1], wqkv.shape[2]
    kc, vc = query.shape[1], value.shape[1]
    Ko, FH = wout.shape[1], wup.shape[2]
    S = qz_s.shape[2]
    S2, S3 = uz_s.shape[1], dz_s.shape[1]
    heads = kc // DK
    g, z, t = lax.axis_index("grp"), lax.axis_index("fs"), lax.axis_index("tp")
    x, c = lax.div(t, 2), lax.rem(t, 2)
    h = lax.rem(z, 2)
    mate = z + 1 - 2 * h
    sends = Sends()

    at_z = lambda other: (g, other, t)
    at_t = lambda other: (g, z, other)
    at_y = (1 - g, z, t)
    at_core = (g, z, t + 1 - 2 * c)
    core = t + 1 - 2 * c

    def arrived(dst, sem, cond=None):
        when(cond, lambda: pltpu.make_async_remote_copy(
            src_ref=dst, dst_ref=dst, send_sem=sem, recv_sem=sem,
            device_id=at_y, device_id_type=MESH,
        ).wait_recv())

    def aligned(value, size):
        return pl.multiple_of(value * size, size)

    copies = [
        pltpu.make_async_copy(query, wqkv.at[z, :, pl.ds(0, kc)], loc.at[0]),
        pltpu.make_async_copy(key, wqkv.at[z, :, pl.ds(kc, kc)], loc.at[1]),
        pltpu.make_async_copy(value, wqkv.at[z, :, pl.ds(2 * kc, vc)], loc.at[2]),
    ]
    tok_copies = [
        pltpu.make_async_copy(tokens.at[:, pl.ds(u * Co, Co)], tokg.at[t * U + u], loc.at[3 + u])
        for u in range(U)
    ]
    late_copies = [
        pltpu.make_async_copy(out_weight, wout.at[z], loc.at[3 + U]),
        pltpu.make_async_copy(up.at[:, pl.ds(aligned(h, FH), FH)], wup.at[z], loc.at[4 + U]),
        pltpu.make_async_copy(down.at[pl.ds(aligned(h, FH), FH), :], wdown.at[z], loc.at[5 + U]),
    ]
    for copy in copies + tok_copies + late_copies:
        copy.start()

    barrier = pltpu.get_barrier_semaphore()
    partners = [at_y]
    partners += [at_z(lax.rem(z + i, F)) for i in range(1, F)]
    partners += [at_t(lax.rem(t + i, T)) for i in range(1, T)]
    for device in partners:
        pl.semaphore_signal(barrier, inc=1, device_id=device, device_id_type=MESH)
    pl.semaphore_wait(barrier, len(partners))

    half = Rz // 2
    step = half // S

    def piece(owner, s, side):
        return wqkv.at[owner, pl.ds(pl.multiple_of(side * half + s * step, step), step), :]

    for copy in copies:
        copy.wait()
    for s in range(S):
        for way, cond in ((0, z < F - 1), (1, z > 0)):
            to = z + 1 - 2 * way
            sends.start(piece(z, s, g), piece(z, s, g), qz_s.at[way, z, s], qz_r.at[z, s], at_z(to), cond)
    for copy in tok_copies:
        copy.wait()
    for i in range(1, T):
        to = lax.rem(t + i, T)
        mine = tokg.at[pl.ds(t * U, U)]
        sends.start(mine, mine, tok_s.at[to], tok_r.at[t], at_t(to))
    def out_piece(owner, side):
        return wout.at[owner, pl.ds(aligned(side, Ko // 2), Ko // 2), :]

    def up_piece(owner, s, side):
        size = Rz // 2 // S2
        return wup.at[owner, pl.ds(pl.multiple_of(side * (Rz // 2) + s * size, size), size), :]

    def columns(s):
        return pl.ds(s * (Co // S3), Co // S3)

    def down_piece(owner, s, side):
        return wdown.at[owner, pl.ds(aligned(side, FH // 2), FH // 2), columns(s)]

    def others(d):
        return ((z + d, z + d < F), (z - d, z >= d))

    def send_up(d, s, ways=(None, None)):
        size = Rz // 2 // S2
        rows = pl.ds(pl.multiple_of(g * (Rz // 2) + s * size, size), size)
        part = lax.rem(h + d, 2)
        for (to, there), way in zip(others(d), ways):
            there = there if way is None else there & way
            sends.start(
                up.at[rows, pl.ds(aligned(part, FH), FH)], up_piece(z, s, g),
                uz_s.at[to, s], uz_r.at[z, s], at_z(to), there,
            )

    def send_down(d, s, ways=(None, None)):
        part = lax.rem(h + d, 2)
        rows = pl.ds(aligned(2 * part + g, FH // 2), FH // 2)
        for (to, there), way in zip(others(d), ways):
            there = there if way is None else there & way
            sends.start(
                down.at[rows, columns(s)], down_piece(z, s, g), dz_s.at[to, s], dz_r.at[z, s], at_z(to),
                there,
            )

    def stream(d, mine_of, send, recv, y_send, y_recv, inner_only):
        for way, (owner, there) in enumerate(((z - d, z >= d), (z + d, z + d < F))):
            onward = there & ((z < F - 1) if way == 0 else (z > 0))
            if inner_only:
                there = onward
            mine, here = mine_of(owner), recv(owner)
            arrived(mine, here, there)
            sends.start(mine, mine, send(way, owner), here, at_z(z + 1 - 2 * way), onward)
            sends.start(mine, mine, y_send(owner), y_recv(owner), at_y, there)

    def stream_late(d):
        steps = []
        for way, (owner, there) in enumerate(((z - d, z >= d), (z + d, z + d < F))):
            inner = (z < F - 1) if way == 0 else (z > 0)
            ends = (z == F - 1) if way == 0 else (z == 0)
            onward = there & inner
            if d <= F // 2:
                there, onward = there & ends, None
            steps.append((
                out_piece(owner, g), oz_r.at[owner], there, onward, oz_s.at[way, owner],
                at_z(z + 1 - 2 * way), oy_s.at[owner], oy_r.at[owner],
            ))

        def event():
            for mine, here, there, onward, send, to, y_send, y_recv in steps:
                arrived(mine, here, there)
                if onward is not None:
                    sends.start(mine, mine, send, here, to, onward)
                sends.start(mine, mine, y_send, y_recv, at_y, there)

        return event

    def stream_qkv(d, s):
        stream(
            d, lambda o: piece(o, s, g), lambda w, o: qz_s.at[w, o, s], lambda o: qz_r.at[o, s],
            lambda o: qy_s.at[o, s], lambda o: qy_r.at[o, s], False,
        )

    def stream_out(d):
        stream(
            d, lambda o: out_piece(o, g), lambda w, o: oz_s.at[w, o], lambda o: oz_r.at[o],
            lambda o: oy_s.at[o], lambda o: oy_r.at[o], True,
        )

    for d in range(1, F):
        for s in range(S):
            stream_qkv(d, s)
        if d == F // 2:
            late_copies[0].wait()
            for way, cond in ((0, z < F - 1), (1, z > 0)):
                mine = out_piece(z, g)
                sends.start(mine, mine, oz_s.at[way, z], oz_r.at[z], at_z(z + 1 - 2 * way), cond)
    for d in range(1, F // 2 + 1):
        stream_out(d)
    even, odd = h == 0, h == 1
    for s in range(S2):
        send_up(1, s)
        send_up(2, s, (even, odd))
    for copy in late_copies[1:]:
        copy.wait()

    def swaps(d, make, z_sem, y_send, y_recv, ways=(None, None)):
        events = []
        for (owner, there), way in zip(others(d), ways):
            there = there if way is None else there & way
            mine, near, send, recv = make(owner), z_sem(owner), y_send(owner), y_recv(owner)

            def event(mine=mine, near=near, send=send, recv=recv, there=there):
                arrived(mine, near, there)
                sends.start(mine, mine, send, recv, at_y, there)

            events.append(event)
        def run():
            for event in events:
                event()

        return run

    def up_swap(d, s):
        return swaps(
            d, lambda o: up_piece(o, s, g), lambda o: uz_r.at[o, s], lambda o: uy_s.at[o, s],
            lambda o: uy_r.at[o, s],
        )

    def down_swap(d, s, ways=(None, None)):
        return swaps(
            d, lambda o: down_piece(o, s, g), lambda o: dz_r.at[o, s], lambda o: dy_s.at[o, s],
            lambda o: dy_r.at[o, s], ways,
        )

    for i in range(1, T):
        owner = lax.rem(t + i, T)
        arrived(tokg.at[pl.ds(owner * U, U)], tok_r.at[owner])
    local_up = decay_up[:, pl.ds(aligned(t, kc), kc)]
    local_bias = decay_bias[:, pl.ds(aligned(t, kc), kc)]

    def decay_rows(rows):
        low = jnp.zeros((BAND, lower.shape[0]), F32)
        for f in range(F):
            low += lax.dot_general(
                tokg[f, rows], lower[:, f * Co : (f + 1) * Co], NT, preferred_element_type=F32
            )
        gate = dot(low.astype(BF16), local_up) + local_bias
        logsig = jnp.minimum(gate, 0.0) - jnp.log1p(jnp.exp(-jnp.abs(gate)))
        decay[rows, :] = logsig / TAU + extra[rows, :]

    loop(R, BAND, decay_rows)

    for i in range(1, F):
        owner = lax.rem(z + i, F)
        for s in range(S):
            arrived(piece(owner, s, 1 - g), qy_r.at[owner, s])

    def qkv_columns(cols):
        total = dot(tokg[0], wqkv[0, :, cols])
        for f in range(1, F):
            total += dot(tokg[f], wqkv[f, :, cols])
        qkv[:, cols] = total.astype(BF16)

    loop(W, TILE, qkv_columns)

    chunks = R // CHUNK
    events = []
    for d in range(1, F):
        events.append((min(chunks - 1, 2 * d - 1), stream_late(d)))
    scan_heads(heads, qkv, decay, head_gain[...], mixed, events)

    for s in range(S2):
        send_up(2, s, (odd, even))
        for d in range(3, F):
            send_up(d, s)
    for s in range(S3):
        send_down(1, s, (odd, even))
    for i in range(1, F):
        owner = lax.rem(z + i, F)
        arrived(out_piece(owner, 1 - g), oy_r.at[owner])
    for i in range(X):
        j = lax.rem(x + 1 + i, X)
        for u in range(U):
            k, block = i * U + u, (2 * j + 1 - c) * U + u

            def other_rows(rows, k=k, block=block):
                mp[k, rows] = dot(mixed[rows], wout[block]).astype(BF16)

            loop(R, TILE, other_rows)
            sends.start(mp.at[k], md.at[k], md_s.at[k], md_r.at[k], at_core)
    for i in range(X):
        j = lax.rem(x + 1 + i, X)
        for u in range(U):
            k, block = i * U + u, (2 * j + c) * U + u
            arrived(md.at[k], md_r.at[k])

            def own_rows(rows, i=i, u=u, k=k, block=block):
                total = dot(mixed[rows], wout[block]) + md[k, rows].astype(F32)
                if i < X - 1:
                    xs[k, rows] = total.astype(BF16)
                else:
                    mk[u, rows] = total

            loop(R, TILE, own_rows)
            if i < X - 1:
                sends.start(xs.at[k], xr.at[x, u], mx_s.at[k], mx_r.at[x, u], at_t(2 * j + c))
    up_swap(1, 0)()

    def share_stats(slot):
        mine = st.at[slot]
        for i in range(1, T):
            to = lax.rem(t + i, T)
            sends.start(mine, sta.at[slot, t], st_s.at[slot, to], st_r.at[slot, t], at_t(to))

    def row_stats(slot, rows, parts):
        ones = jnp.ones((8, Co), F32)
        for kind in range(2):
            total = None
            for part in parts:
                term = lax.dot_general(
                    ones, part * part if kind else part, NT,
                    precision=lax.Precision.HIGHEST, preferred_element_type=F32,
                )
                total = term if total is None else total + term
            st[slot, kind, :, rows] = total
            sta[slot, t, kind, :, rows] = total

    def await_stats(slot):
        for i in range(1, T):
            owner = lax.rem(t + i, T)
            arrived(sta.at[slot, owner], st_r.at[slot, owner])

    def scale_of(slot, rows):
        totals = []
        for kind in range(2):
            total = sta[slot, 0, kind, :, rows]
            for other in range(1, T):
                total += sta[slot, other, kind, :, rows]
            totals.append(total / (Co * F))
        mean = totals[0]
        scale = lax.rsqrt(totals[1] - mean * mean + EPS)
        return mean.T[:, 0:1], scale.T[:, 0:1]

    for i in range(1, X):
        j = lax.rem(x + i, X)
        for u in range(U):
            arrived(xr.at[j, u], mx_r.at[j, u])

    def mix_rows(rows):
        parts = []
        for u in range(U):
            total = mk[u, rows]
            for i in range(1, X):
                total += xr[lax.rem(x + i, X), u, rows].astype(F32)
            total += ALPHA * tokg[t * U + u, rows].astype(F32)
            v[u, rows] = total
            parts.append(total)
        row_stats(0, rows, parts)

    loop(R, BAND, mix_rows)
    share_stats(0)
    await_stats(0)

    def norm_rows(rows):
        mean, scale = scale_of(0, rows)
        for u in range(U):
            gain = mix_gain[:, u * Co : (u + 1) * Co]
            normg[h, t * U + u, rows] = ((v[u, rows] - mean) * scale * gain).astype(BF16)

    loop(R, BAND, norm_rows)

    def region(pair, owner):
        return normg.at[pair, pl.ds(owner * U, U)]

    def forward(pair, owner, slot, device):
        mine = region(pair, owner)
        sends.start(mine, mine, nm_s.at[pair, owner, slot], nm_r.at[pair, owner], device)

    def await_region(pair, owner):
        arrived(region(pair, owner), nm_r.at[pair, owner])

    forward(h, t, X, at_z(mate))
    for i in range(1, X):
        forward(h, t, i, at_t(2 * lax.rem(x + i, X) + c))
    forward(h, t, 0, at_core)
    for s in range(S3):
        send_down(1, s, (even, odd))
        send_down(2, s, (even, odd))
    for s in range(1, S2):
        up_swap(1, s)()
    for s in range(S2):
        for d in range(2, F):
            up_swap(d, s)()
    await_region(1 - h, t)
    for i in range(1, X):
        forward(1 - h, t, i, at_t(2 * lax.rem(x + i, X) + c))
    forward(1 - h, t, 0, at_core)
    ends = (z == 0) | (z == F - 1)
    inside = (z > 0) & (z < F - 1)

    def send_far(only):
        for s in range(S3):
            send_down(2, s, (odd & only, even & only))
            for d in range(3, F):
                send_down(d, s, (only, only))

    for s in range(S3):
        down_swap(1, s, (odd, even))()
        down_swap(1, s, (even & ends, odd & ends))()
        if s == 0:
            send_far(ends)
    for i in range(1, X):
        owner = 2 * lax.rem(x + i, X) + c
        await_region(h, owner)
        forward(h, owner, 0, at_core)
    for i in range(1, F):
        owner = lax.rem(z + i, F)
        for s in range(S2):
            arrived(up_piece(owner, s, 1 - g), uy_r.at[owner, s])

    def hidden(pair):
        for i in range(X):
            await_region(pair, 2 * lax.rem(x + i, X) + 1 - c)

        def hidden_columns(cols):
            total = dot(normg[pair, 0], wup[0, :, cols])
            for f in range(1, F):
                total += dot(normg[pair, f], wup[f, :, cols])
            act[pair, :, cols] = jnp.square(jnp.maximum(total, 0.0)).astype(BF16)

        loop(FH, TILE, hidden_columns)

    send_far(inside)
    hidden(h)
    for s in range(S3):
        down_swap(1, s, (even & inside, odd & inside))()
    for i in range(1, X):
        owner = 2 * lax.rem(x + i, X) + c
        await_region(1 - h, owner)
        forward(1 - h, owner, 0, at_core)
    late = [(d, s) for s in range(S3) for d in range(2, F)]
    hidden(1 - h)
    if U == 1:
        for d in range(2, F):
            down_swap(d, 0)()

    pair_of = lax.div(z, 2)
    bands = [pl.ds(r * BAND, BAND) for r in range(R // BAND)]

    def await_down(block, s):
        arrived(down_piece(block, s, 1 - g), dy_r.at[block, s], block != z)

    def project(i, j, u, s):
        k, cols = i * U + u, columns(s)
        block = (2 * j + 1 - c) * U + u
        for slot, pair in enumerate((1 - h, h)):

            def other_rows(rows, block=block, slot=slot, pair=pair):
                dnp[k, slot, rows, cols] = dot(act[pair, rows], wdown[block, :, cols]).astype(BF16)

            loop(R, TILE, other_rows)
            mine = (k, slot, slice(None), cols)
            sends.start(
                dnp.at[mine], dnd.at[mine], dd_s.at[k, slot, s], dd_r.at[k, slot, s], at_core
            )
        block = (2 * j + c) * U + u
        arrived(dnd.at[k, 0, :, cols], dd_r.at[k, 0, s])
        for r, rows in enumerate(bands):
            total = dot(act[1 - h, rows], wdown[block, :, cols])
            dzs[k, rows, cols] = (total + dnd[k, 0, rows, cols].astype(F32)).astype(BF16)
            sends.start(
                dzs.at[k, rows, cols], dzr.at[k, rows, cols], dp_s.at[k, r, s], dp_r.at[k, r, s],
                at_z(mate),
            )
        arrived(dnd.at[k, 1, :, cols], dd_r.at[k, 1, s])

        def own_rows(rows, block=block):
            total = dot(act[h, rows], wdown[block, :, cols])
            ck[k, rows, cols] = total + dnd[k, 1, rows, cols].astype(F32)

        loop(R, TILE, own_rows)

    def add_pair(i, j, u, s):
        k, cols = i * U + u, columns(s)
        for r, rows in enumerate(bands):
            arrived(dzr.at[k, rows, cols], dp_r.at[k, r, s])
            total = ck[k, rows, cols] + dzr[k, rows, cols].astype(F32)
            dxs[k, rows, cols] = total.astype(BF16)
            sends.start(
                dxs.at[k, rows, cols], dxr.at[x, u, rows, cols], dx_s.at[k, r, s],
                dx_r.at[x, u, r, s], at_t(2 * j + c), j != x,
            )

    if U > 1:
        for s in range(S3):
            for d in range(2, F):
                down_swap(d, s)()
    for i in range(X):
        j = lax.rem(pair_of + i, X)
        for s in range(S3):
            for block in range(2 * U):
                await_down(2 * j * U + block, s)
            for u in range(U):
                project(i, j, u, s)
            if i == 0 and U == 1 and s > 0:
                for d in range(2, F):
                    down_swap(d, s)()
            if i > 0 and s == 0:
                for part in range(S3):
                    for u in range(U):
                        add_pair(i - 1, lax.rem(pair_of + i - 1, X), u, part)
            if i == X - 1 and s < S3 - 1:
                for u in range(U):
                    add_pair(i, j, u, s)
    j = lax.rem(pair_of + X - 1, X)
    for u in range(U):
        add_pair(X - 1, j, u, S3 - 1)
    for i in range(1, X):
        j = lax.rem(x + i, X)
        for u in range(U):
            for s in range(S3):
                for r, rows in enumerate(bands):
                    arrived(dxr.at[j, u, rows, columns(s)], dx_r.at[j, u, r, s])
    own = lax.rem(x - lax.rem(pair_of, X) + X, X) * U

    def last_rows(rows):
        parts = []
        for u in range(U):
            total = ck[own + u, rows] + dzr[own + u, rows].astype(F32)
            for i in range(1, X):
                total += dxr[lax.rem(x + i, X), u, rows].astype(F32)
            total += ALPHA * normg[h, t * U + u, rows].astype(F32)
            v[u, rows] = total
            parts.append(total)
        row_stats(1, rows, parts)

    loop(R, BAND, last_rows)
    share_stats(1)
    await_stats(1)

    def result_rows(rows):
        mean, scale = scale_of(1, rows)
        for u in range(U):
            gain = out_gain[:, u * Co : (u + 1) * Co]
            result[rows, u * Co : (u + 1) * Co] = ((v[u, rows] - mean) * scale * gain).astype(BF16)

    loop(R, BAND, result_rows)
    sends.drain()


def local(F, T, *args):
    (tokens, query, key, value, lower, decay_up, decay_bias, extra, head_gain, out_weight,
     mix_gain, up, down, out_gain) = args
    U, X = F // T, T // 2
    R, Dt = tokens.shape
    Co = Dt // U
    Rz, kc = query.shape
    W = 2 * kc + value.shape[1]
    Ko = out_weight.shape[0]
    FH = up.shape[1] // 2
    heads = kc // DK
    S, S2, S3 = 2, 2, 2 if Co % (2 * DK) == 0 else 1
    vmem, hbm = pl.BlockSpec(memory_space=pltpu.VMEM), pl.BlockSpec(memory_space=pl.ANY)
    sem = lambda *shape: pltpu.SemaphoreType.DMA(shape)
    buf = lambda *shape: pltpu.VMEM(shape, BF16)
    wide = lambda *shape: pltpu.VMEM(shape, F32)
    H = X * U
    scratch = [
        buf(F, R, Co), buf(F, Rz, W), buf(F, Ko, Co), buf(F, Rz, FH), buf(F, FH, Co),
        buf(R, W), wide(R, kc), buf(R, heads * DV),
        buf(H, R, Co), buf(H, R, Co), buf(H, R, Co), buf(X, U, R, Co), wide(U, R, Co),
        wide(U, R, Co), wide(2, 2, 8, R), wide(2, T, 2, 8, R), buf(2, F, R, Co), buf(2, R, FH),
        buf(H, 2, R, Co), buf(H, 2, R, Co), wide(H, R, Co), buf(H, R, Co), buf(H, R, Co),
        buf(H, R, Co), buf(X, U, R, Co),
        sem(6 + U), sem(T), sem(T), sem(2, F, S), sem(F, S), sem(F, S), sem(F, S),
        sem(2, F), sem(F), sem(F), sem(F),
        sem(F, S2), sem(F, S2), sem(F, S2), sem(F, S2),
        sem(F, S3), sem(F, S3), sem(F, S3), sem(F, S3),
        sem(H), sem(H), sem(H), sem(X, U), sem(2, T), sem(2, T), sem(2, T, X + 1), sem(2, T),
        sem(H, 2, S3), sem(H, 2, S3), sem(H, R // BAND, S3), sem(H, R // BAND, S3),
        sem(H, R // BAND, S3), sem(X, U, R // BAND, S3),
    ]
    return pl.pallas_call(
        functools.partial(kernel, F, T),
        out_shape=jax.ShapeDtypeStruct((R, Dt), BF16),
        in_specs=[hbm, hbm, hbm, hbm, vmem, vmem, vmem, vmem, vmem, hbm, vmem, hbm, hbm, vmem],
        out_specs=vmem,
        scratch_shapes=scratch,
        compiler_params=pltpu.CompilerParams(
            collective_id=0, has_side_effects=True, vmem_limit_bytes=63 * 2**20
        ),
        name="layer",
    )(
        tokens, query, key, value, lower.T, decay_up, decay_bias[None], extra, head_gain[None],
        out_weight, mix_gain[None], up, down, out_gain[None],
    )


def solution(mesh):
    in_specs = (
        P(("grp", "fs"), "tp"),
        P("fs", "tp"),
        P("fs", "tp"),
        P("fs", "tp"),
        P(),
        P(),
        P(),
        P(("grp", "fs"), "tp"),
        P(),
        P("tp", "fs"),
        P("tp"),
        P("fs", "tp"),
        P("tp", "fs"),
        P("tp"),
    )
    out_specs = P(("grp", "fs"), "tp")
    body = functools.partial(local, mesh.shape["fs"], mesh.shape["tp"])
    return jax.shard_map(body, mesh=mesh, in_specs=in_specs, out_specs=out_specs, check_vma=False)
```

```python
import functools

import jax
import jax.numpy as jnp
from jax import lax
from jax.experimental import pallas as pl
from jax.experimental.pallas import tpu as pltpu
from jax.sharding import PartitionSpec as P

DK = 128
DV = 256
CHUNK = 64
SUB = 16
TILE = 256
BAND = 128

ALPHA = 2.0**0.5
TAU = 16.0
EPS = 1e-05

MESH = pl.DeviceIdType.MESH
NT = (((1,), (1,)), ((), ()))
TN = (((0,), (0,)), ((), ()))
BF16, F32 = jnp.bfloat16, jnp.float32


def dot(a, b):
    return jnp.dot(a, b, preferred_element_type=F32)


def loop(count, size, body):
    def step(index, carry):
        body(pl.ds(pl.multiple_of(index * size, size), size))
        return carry

    lax.fori_loop(0, count // size, step, 0)


def when(cond, body):
    if cond is None:
        body()
    else:
        pl.when(cond)(body)


class Sends:
    def __init__(self):
        self.open = []

    def start(self, src, dst, send, recv, device, cond=None):
        def copy():
            return pltpu.make_async_remote_copy(
                src_ref=src, dst_ref=dst, send_sem=send, recv_sem=recv,
                device_id=device, device_id_type=MESH,
            )

        when(cond, lambda: copy().start())
        self.open.append((cond, copy))

    def drain(self):
        for cond, copy in self.open:
            when(cond, lambda copy=copy: copy().wait_send())
        self.open = []


def scan_heads(heads, qkv_ref, decay_ref, gain, out_ref, events):
    rows = qkv_ref.shape[0]
    at_row = lax.broadcasted_iota(jnp.int32, (CHUNK, CHUNK), 0)
    at_col = lax.broadcasted_iota(jnp.int32, (CHUNK, CHUNK), 1)
    tri = (at_row >= at_col).astype(F32)
    sub_row = lax.broadcasted_iota(jnp.int32, (SUB, SUB), 0)
    sub_col = lax.broadcasted_iota(jnp.int32, (SUB, SUB), 1)

    def step(index, states):
        for at, event in events:
            pl.when(index == at)(event)
        here = pl.ds(pl.multiple_of(index * CHUNK, CHUNK), CHUNK)
        fresh_states = []
        for head in range(heads):
            query = qkv_ref[here, head * DK : (head + 1) * DK].astype(F32) * DK**-0.5
            keys = qkv_ref[here, (heads + head) * DK : (heads + head + 1) * DK].astype(F32)
            at_value = 2 * heads * DK + head * DV
            value = qkv_ref[here, at_value : at_value + DV]
            decay = decay_ref[here, head * DK : (head + 1) * DK]
            cumul = jnp.dot(
                tri, decay, precision=lax.Precision.HIGHEST, preferred_element_type=F32
            )
            last = cumul[CHUNK - 1 : CHUNK, :]
            state = states[head]
            out = lax.dot_general(
                (query * jnp.exp(cumul)).astype(BF16),
                state.astype(BF16),
                NT,
                preferred_element_type=F32,
            )
            strips = []
            for a in range(CHUNK // SUB):
                lo, hi = a * SUB, (a + 1) * SUB
                q_a, k_a, g_a = query[lo:hi], keys[lo:hi], cumul[lo:hi]
                diag = jnp.zeros((SUB, SUB), F32)
                for j in range(SUB):
                    weight = jnp.exp(jnp.minimum(g_a - g_a[j : j + 1], 0.0))
                    column = jnp.sum(q_a * k_a[j : j + 1] * weight, axis=1, keepdims=True)
                    diag = jnp.where((sub_col == j) & (sub_row >= j), column, diag)
                strip = dot(diag.astype(BF16), value[lo:hi])
                if a:
                    base = cumul[lo - 1 : lo]
                    before = lax.dot_general(
                        (q_a * jnp.exp(g_a - base)).astype(BF16),
                        (keys[:lo] * jnp.exp(base - cumul[:lo])).astype(BF16),
                        NT,
                        preferred_element_type=F32,
                    )
                    strip += dot(before.astype(BF16), value[:lo])
                strips.append(strip)
            out = out + jnp.concatenate(strips, axis=0)
            fresh = lax.dot_general(
                value,
                (keys * jnp.exp(last - cumul)).astype(BF16),
                TN,
                preferred_element_type=F32,
            )
            fresh_states.append(state * jnp.exp(last) + fresh)
            mean = jnp.mean(out * out, axis=1, keepdims=True)
            out_ref[here, head * DV : (head + 1) * DV] = (
                out * lax.rsqrt(mean + EPS) * gain
            ).astype(BF16)
        return tuple(fresh_states)

    start = tuple(jnp.zeros((DV, DK), F32) for _ in range(heads))
    lax.fori_loop(0, rows // CHUNK, step, start)


def kernel(
    F, T,
    tokens, query, key, value, lower, decay_up, decay_bias, extra, head_gain, out_weight,
    mix_gain, up, down, out_gain,
    result,
    tokg, wqkv, wout, wup, wdown, qkv, decay, mixed, mp, md, xs, xr, mk, v, st, sta, normg, act,
    dnp, dnd, ck, dzs, dzr, dxs, dxr,
    loc, tok_s, tok_r, qz_s, qz_r, qy_s, qy_r, oz_s, oz_r, oy_s, oy_r, uz_s, uz_r, uy_s, uy_r,
    dz_s, dz_r, dy_s, dy_r, md_s, md_r, mx_s, mx_r, st_s, st_r, nm_s, nm_r, dd_s, dd_r,
    dp_s, dp_r, dx_s, dx_r,
):
    U, X = F // T, T // 2
    R, Co = v.shape[1], v.shape[2]
    Rz, W = wqkv.shape[1], wqkv.shape[2]
    kc, vc = query.shape[1], value.shape[1]
    Ko, FH = wout.shape[1], wup.shape[2]
    S = qz_s.shape[2]
    S2, S3 = uz_s.shape[1], dz_s.shape[1]
    heads = kc // DK
    g, z, t = lax.axis_index("grp"), lax.axis_index("fs"), lax.axis_index("tp")
    x, c = lax.div(t, 2), lax.rem(t, 2)
    h = lax.rem(z, 2)
    mate = z + 1 - 2 * h
    sends = Sends()

    at_z = lambda other: (g, other, t)
    at_t = lambda other: (g, z, other)
    at_y = (1 - g, z, t)
    at_core = (g, z, t + 1 - 2 * c)
    core = t + 1 - 2 * c

    def arrived(dst, sem, cond=None):
        when(cond, lambda: pltpu.make_async_remote_copy(
            src_ref=dst, dst_ref=dst, send_sem=sem, recv_sem=sem,
            device_id=at_y, device_id_type=MESH,
        ).wait_recv())

    def aligned(value, size):
        return pl.multiple_of(value * size, size)

    copies = [
        pltpu.make_async_copy(query, wqkv.at[z, :, pl.ds(0, kc)], loc.at[0]),
        pltpu.make_async_copy(key, wqkv.at[z, :, pl.ds(kc, kc)], loc.at[1]),
        pltpu.make_async_copy(value, wqkv.at[z, :, pl.ds(2 * kc, vc)], loc.at[2]),
    ]
    tok_copies = [
        pltpu.make_async_copy(tokens.at[:, pl.ds(u * Co, Co)], tokg.at[t * U + u], loc.at[3 + u])
        for u in range(U)
    ]
    late_copies = [
        pltpu.make_async_copy(out_weight, wout.at[z], loc.at[3 + U]),
        pltpu.make_async_copy(up.at[:, pl.ds(aligned(h, FH), FH)], wup.at[z], loc.at[4 + U]),
        pltpu.make_async_copy(down.at[pl.ds(aligned(h, FH), FH), :], wdown.at[z], loc.at[5 + U]),
    ]
    for copy in copies + tok_copies + late_copies:
        copy.start()

    barrier = pltpu.get_barrier_semaphore()
    partners = [at_y]
    partners += [at_z(lax.rem(z + i, F)) for i in range(1, F)]
    partners += [at_t(lax.rem(t + i, T)) for i in range(1, T)]
    for device in partners:
        pl.semaphore_signal(barrier, inc=1, device_id=device, device_id_type=MESH)
    pl.semaphore_wait(barrier, len(partners))

    half = Rz // 2
    step = half // S

    def piece(owner, s, side):
        return wqkv.at[owner, pl.ds(pl.multiple_of(side * half + s * step, step), step), :]

    for copy in copies:
        copy.wait()
    for s in range(S):
        for way, cond in ((0, z < F - 1), (1, z > 0)):
            to = z + 1 - 2 * way
            sends.start(piece(z, s, g), piece(z, s, g), qz_s.at[way, z, s], qz_r.at[z, s], at_z(to), cond)
    for copy in tok_copies:
        copy.wait()
    for i in range(1, T):
        to = lax.rem(t + i, T)
        mine = tokg.at[pl.ds(t * U, U)]
        sends.start(mine, mine, tok_s.at[to], tok_r.at[t], at_t(to))
    def out_piece(owner, side):
        return wout.at[owner, pl.ds(aligned(side, Ko // 2), Ko // 2), :]

    def up_piece(owner, s, side):
        size = Rz // 2 // S2
        return wup.at[owner, pl.ds(pl.multiple_of(side * (Rz // 2) + s * size, size), size), :]

    def columns(s):
        return pl.ds(s * (Co // S3), Co // S3)

    def down_piece(owner, s, side):
        return wdown.at[owner, pl.ds(aligned(side, FH // 2), FH // 2), columns(s)]

    def others(d):
        return ((z + d, z + d < F), (z - d, z >= d))

    def send_up(d, s, ways=(None, None)):
        size = Rz // 2 // S2
        rows = pl.ds(pl.multiple_of(g * (Rz // 2) + s * size, size), size)
        part = lax.rem(h + d, 2)
        for (to, there), way in zip(others(d), ways):
            there = there if way is None else there & way
            sends.start(
                up.at[rows, pl.ds(aligned(part, FH), FH)], up_piece(z, s, g),
                uz_s.at[to, s], uz_r.at[z, s], at_z(to), there,
            )

    def send_down(d, s, ways=(None, None)):
        part = lax.rem(h + d, 2)
        rows = pl.ds(aligned(2 * part + g, FH // 2), FH // 2)
        for (to, there), way in zip(others(d), ways):
            there = there if way is None else there & way
            sends.start(
                down.at[rows, columns(s)], down_piece(z, s, g), dz_s.at[to, s], dz_r.at[z, s], at_z(to),
                there,
            )

    def stream(d, mine_of, send, recv, y_send, y_recv, inner_only):
        for way, (owner, there) in enumerate(((z - d, z >= d), (z + d, z + d < F))):
            onward = there & ((z < F - 1) if way == 0 else (z > 0))
            if inner_only:
                there = onward
            mine, here = mine_of(owner), recv(owner)
            arrived(mine, here, there)
            sends.start(mine, mine, send(way, owner), here, at_z(z + 1 - 2 * way), onward)
            sends.start(mine, mine, y_send(owner), y_recv(owner), at_y, there)

    def stream_late(d):
        steps = []
        for way, (owner, there) in enumerate(((z - d, z >= d), (z + d, z + d < F))):
            inner = (z < F - 1) if way == 0 else (z > 0)
            ends = (z == F - 1) if way == 0 else (z == 0)
            onward = there & inner
            if d <= F // 2:
                there, onward = there & ends, None
            steps.append((
                out_piece(owner, g), oz_r.at[owner], there, onward, oz_s.at[way, owner],
                at_z(z + 1 - 2 * way), oy_s.at[owner], oy_r.at[owner],
            ))

        def event():
            for mine, here, there, onward, send, to, y_send, y_recv in steps:
                arrived(mine, here, there)
                if onward is not None:
                    sends.start(mine, mine, send, here, to, onward)
                sends.start(mine, mine, y_send, y_recv, at_y, there)

        return event

    def stream_qkv(d, s):
        stream(
            d, lambda o: piece(o, s, g), lambda w, o: qz_s.at[w, o, s], lambda o: qz_r.at[o, s],
            lambda o: qy_s.at[o, s], lambda o: qy_r.at[o, s], False,
        )

    def stream_out(d):
        stream(
            d, lambda o: out_piece(o, g), lambda w, o: oz_s.at[w, o], lambda o: oz_r.at[o],
            lambda o: oy_s.at[o], lambda o: oy_r.at[o], True,
        )

    for d in range(1, F):
        for s in range(S):
            stream_qkv(d, s)
        if d == F // 2:
            late_copies[0].wait()
            for way, cond in ((0, z < F - 1), (1, z > 0)):
                mine = out_piece(z, g)
                sends.start(mine, mine, oz_s.at[way, z], oz_r.at[z], at_z(z + 1 - 2 * way), cond)
    for d in range(1, F // 2 + 1):
        stream_out(d)
    even, odd = h == 0, h == 1
    for s in range(S2):
        send_up(1, s)
        send_up(2, s, (even, odd))
    for copy in late_copies[1:]:
        copy.wait()

    def swaps(d, make, z_sem, y_send, y_recv, ways=(None, None)):
        events = []
        for (owner, there), way in zip(others(d), ways):
            there = there if way is None else there & way
            mine, near, send, recv = make(owner), z_sem(owner), y_send(owner), y_recv(owner)

            def event(mine=mine, near=near, send=send, recv=recv, there=there):
                arrived(mine, near, there)
                sends.start(mine, mine, send, recv, at_y, there)

            events.append(event)
        def run():
            for event in events:
                event()

        return run

    def up_swap(d, s):
        return swaps(
            d, lambda o: up_piece(o, s, g), lambda o: uz_r.at[o, s], lambda o: uy_s.at[o, s],
            lambda o: uy_r.at[o, s],
        )

    def down_swap(d, s, ways=(None, None)):
        return swaps(
            d, lambda o: down_piece(o, s, g), lambda o: dz_r.at[o, s], lambda o: dy_s.at[o, s],
            lambda o: dy_r.at[o, s], ways,
        )

    for i in range(1, T):
        owner = lax.rem(t + i, T)
        arrived(tokg.at[pl.ds(owner * U, U)], tok_r.at[owner])
    local_up = decay_up[:, pl.ds(aligned(t, kc), kc)]
    local_bias = decay_bias[:, pl.ds(aligned(t, kc), kc)]

    def decay_rows(rows):
        low = jnp.zeros((BAND, lower.shape[0]), F32)
        for f in range(F):
            low += lax.dot_general(
                tokg[f, rows], lower[:, f * Co : (f + 1) * Co], NT, preferred_element_type=F32
            )
        gate = dot(low.astype(BF16), local_up) + local_bias
        logsig = jnp.minimum(gate, 0.0) - jnp.log1p(jnp.exp(-jnp.abs(gate)))
        decay[rows, :] = logsig / TAU + extra[rows, :]

    loop(R, BAND, decay_rows)

    for i in range(1, F):
        owner = lax.rem(z + i, F)
        for s in range(S):
            arrived(piece(owner, s, 1 - g), qy_r.at[owner, s])

    def qkv_columns(cols):
        total = dot(tokg[0], wqkv[0, :, cols])
        for f in range(1, F):
            total += dot(tokg[f], wqkv[f, :, cols])
        qkv[:, cols] = total.astype(BF16)

    loop(W, TILE, qkv_columns)

    chunks = R // CHUNK
    events = []
    for d in range(1, F):
        events.append((min(chunks - 1, 2 * d - 1), stream_late(d)))
    scan_heads(heads, qkv, decay, head_gain[...], mixed, events)

    for s in range(S2):
        send_up(2, s, (odd, even))
        for d in range(3, F):
            send_up(d, s)
    for s in range(S3):
        send_down(1, s, (odd, even))
    for i in range(1, F):
        owner = lax.rem(z + i, F)
        arrived(out_piece(owner, 1 - g), oy_r.at[owner])
    for i in range(X):
        j = lax.rem(x + 1 + i, X)
        for u in range(U):
            k, block = i * U + u, (2 * j + 1 - c) * U + u

            def other_rows(rows, k=k, block=block):
                mp[k, rows] = dot(mixed[rows], wout[block]).astype(BF16)

            loop(R, TILE, other_rows)
            sends.start(mp.at[k], md.at[k], md_s.at[k], md_r.at[k], at_core)
    for i in range(X):
        j = lax.rem(x + 1 + i, X)
        for u in range(U):
            k, block = i * U + u, (2 * j + c) * U + u
            arrived(md.at[k], md_r.at[k])

            def own_rows(rows, i=i, u=u, k=k, block=block):
                total = dot(mixed[rows], wout[block]) + md[k, rows].astype(F32)
                if i < X - 1:
                    xs[k, rows] = total.astype(BF16)
                else:
                    mk[u, rows] = total

            loop(R, TILE, own_rows)
            if i < X - 1:
                sends.start(xs.at[k], xr.at[x, u], mx_s.at[k], mx_r.at[x, u], at_t(2 * j + c))
    up_swap(1, 0)()

    def share_stats(slot):
        mine = st.at[slot]
        for i in range(1, T):
            to = lax.rem(t + i, T)
            sends.start(mine, sta.at[slot, t], st_s.at[slot, to], st_r.at[slot, t], at_t(to))

    def row_stats(slot, rows, parts):
        ones = jnp.ones((8, Co), F32)
        for kind in range(2):
            total = None
            for part in parts:
                term = lax.dot_general(
                    ones, part * part if kind else part, NT,
                    precision=lax.Precision.HIGHEST, preferred_element_type=F32,
                )
                total = term if total is None else total + term
            st[slot, kind, :, rows] = total
            sta[slot, t, kind, :, rows] = total

    def await_stats(slot):
        for i in range(1, T):
            owner = lax.rem(t + i, T)
            arrived(sta.at[slot, owner], st_r.at[slot, owner])

    def scale_of(slot, rows):
        totals = []
        for kind in range(2):
            total = sta[slot, 0, kind, :, rows]
            for other in range(1, T):
                total += sta[slot, other, kind, :, rows]
            totals.append(total / (Co * F))
        mean = totals[0]
        scale = lax.rsqrt(totals[1] - mean * mean + EPS)
        return mean.T[:, 0:1], scale.T[:, 0:1]

    for i in range(1, X):
        j = lax.rem(x + i, X)
        for u in range(U):
            arrived(xr.at[j, u], mx_r.at[j, u])

    def mix_rows(rows):
        parts = []
        for u in range(U):
            total = mk[u, rows]
            for i in range(1, X):
                total += xr[lax.rem(x + i, X), u, rows].astype(F32)
            total += ALPHA * tokg[t * U + u, rows].astype(F32)
            v[u, rows] = total
            parts.append(total)
        row_stats(0, rows, parts)

    loop(R, BAND, mix_rows)
    share_stats(0)
    await_stats(0)

    def norm_rows(rows):
        mean, scale = scale_of(0, rows)
        for u in range(U):
            gain = mix_gain[:, u * Co : (u + 1) * Co]
            normg[h, t * U + u, rows] = ((v[u, rows] - mean) * scale * gain).astype(BF16)

    loop(R, BAND, norm_rows)

    def region(pair, owner):
        return normg.at[pair, pl.ds(owner * U, U)]

    def forward(pair, owner, slot, device):
        mine = region(pair, owner)
        sends.start(mine, mine, nm_s.at[pair, owner, slot], nm_r.at[pair, owner], device)

    def await_region(pair, owner):
        arrived(region(pair, owner), nm_r.at[pair, owner])

    forward(h, t, X, at_z(mate))
    for i in range(1, X):
        forward(h, t, i, at_t(2 * lax.rem(x + i, X) + c))
    forward(h, t, 0, at_core)
    for s in range(S3):
        send_down(1, s, (even, odd))
        send_down(2, s, (even, odd))
    for s in range(1, S2):
        up_swap(1, s)()
    for s in range(S2):
        for d in range(2, F):
            up_swap(d, s)()
    await_region(1 - h, t)
    for i in range(1, X):
        forward(1 - h, t, i, at_t(2 * lax.rem(x + i, X) + c))
    forward(1 - h, t, 0, at_core)
    ends = (z == 0) | (z == F - 1)
    inside = (z > 0) & (z < F - 1)

    def send_far(only):
        for s in range(S3):
            send_down(2, s, (odd & only, even & only))
            for d in range(3, F):
                send_down(d, s, (only, only))

    for s in range(S3):
        down_swap(1, s, (odd, even))()
        down_swap(1, s, (even & ends, odd & ends))()
        if s == 0:
            send_far(ends)
    for i in range(1, X):
        owner = 2 * lax.rem(x + i, X) + c
        await_region(h, owner)
        forward(h, owner, 0, at_core)
    for i in range(1, F):
        owner = lax.rem(z + i, F)
        for s in range(S2):
            arrived(up_piece(owner, s, 1 - g), uy_r.at[owner, s])

    def hidden(pair):
        for i in range(X):
            await_region(pair, 2 * lax.rem(x + i, X) + 1 - c)

        def hidden_columns(cols):
            total = dot(normg[pair, 0], wup[0, :, cols])
            for f in range(1, F):
                total += dot(normg[pair, f], wup[f, :, cols])
            act[pair, :, cols] = jnp.square(jnp.maximum(total, 0.0)).astype(BF16)

        loop(FH, TILE, hidden_columns)

    send_far(inside)
    hidden(h)
    for s in range(S3):
        down_swap(1, s, (even & inside, odd & inside))()
    for i in range(1, X):
        owner = 2 * lax.rem(x + i, X) + c
        await_region(1 - h, owner)
        forward(1 - h, owner, 0, at_core)
    late = [(d, s) for s in range(S3) for d in range(2, F)]
    hidden(1 - h)
    if U == 1:
        for d in range(2, F):
            down_swap(d, 0)()

    pair_of = lax.div(z, 2)
    bands = [pl.ds(r * BAND, BAND) for r in range(R // BAND)]

    def await_down(block, s):
        arrived(down_piece(block, s, 1 - g), dy_r.at[block, s], block != z)

    def project(i, j, u, s):
        k, cols = i * U + u, columns(s)
        block = (2 * j + 1 - c) * U + u
        for slot, pair in enumerate((1 - h, h)):

            def other_rows(rows, block=block, slot=slot, pair=pair):
                dnp[k, slot, rows, cols] = dot(act[pair, rows], wdown[block, :, cols]).astype(BF16)

            loop(R, TILE, other_rows)
            mine = (k, slot, slice(None), cols)
            sends.start(
                dnp.at[mine], dnd.at[mine], dd_s.at[k, slot, s], dd_r.at[k, slot, s], at_core
            )
        block = (2 * j + c) * U + u
        arrived(dnd.at[k, 0, :, cols], dd_r.at[k, 0, s])
        for r, rows in enumerate(bands):
            total = dot(act[1 - h, rows], wdown[block, :, cols])
            dzs[k, rows, cols] = (total + dnd[k, 0, rows, cols].astype(F32)).astype(BF16)
            sends.start(
                dzs.at[k, rows, cols], dzr.at[k, rows, cols], dp_s.at[k, r, s], dp_r.at[k, r, s],
                at_z(mate),
            )
        arrived(dnd.at[k, 1, :, cols], dd_r.at[k, 1, s])

        def own_rows(rows, block=block):
            total = dot(act[h, rows], wdown[block, :, cols])
            ck[k, rows, cols] = total + dnd[k, 1, rows, cols].astype(F32)

        loop(R, TILE, own_rows)

    def add_pair(i, j, u, s):
        k, cols = i * U + u, columns(s)
        for r, rows in enumerate(bands):
            arrived(dzr.at[k, rows, cols], dp_r.at[k, r, s])
            total = ck[k, rows, cols] + dzr[k, rows, cols].astype(F32)
            dxs[k, rows, cols] = total.astype(BF16)
            sends.start(
                dxs.at[k, rows, cols], dxr.at[x, u, rows, cols], dx_s.at[k, r, s],
                dx_r.at[x, u, r, s], at_t(2 * j + c), j != x,
            )

    if U > 1:
        for s in range(S3):
            for d in range(2, F):
                down_swap(d, s)()
    for i in range(X):
        j = lax.rem(pair_of + i, X)
        for s in range(S3):
            for block in range(2 * U):
                await_down(2 * j * U + block, s)
            for u in range(U):
                project(i, j, u, s)
            if i == 0 and U == 1 and s > 0:
                for d in range(2, F):
                    down_swap(d, s)()
            if i > 0 and s == 0:
                for part in range(S3):
                    for u in range(U):
                        add_pair(i - 1, lax.rem(pair_of + i - 1, X), u, part)
            if i == X - 1 and s < S3 - 1:
                for u in range(U):
                    add_pair(i, j, u, s)
    j = lax.rem(pair_of + X - 1, X)
    for u in range(U):
        add_pair(X - 1, j, u, S3 - 1)
    own = lax.rem(x - lax.rem(pair_of, X) + X, X) * U

    def last_rows(rows):
        parts = []
        for u in range(U):
            total = ck[own + u, rows] + dzr[own + u, rows].astype(F32)
            for i in range(1, X):
                total += dxr[lax.rem(x + i, X), u, rows].astype(F32)
            total += ALPHA * normg[h, t * U + u, rows].astype(F32)
            v[u, rows] = total
            parts.append(total)
        row_stats(1, rows, parts)

    for r, rows in enumerate(bands):
        for i in range(1, X):
            j = lax.rem(x + i, X)
            for u in range(U):
                for s in range(S3):
                    arrived(dxr.at[j, u, rows, columns(s)], dx_r.at[j, u, r, s])
        last_rows(rows)
    share_stats(1)
    await_stats(1)

    def result_rows(rows):
        mean, scale = scale_of(1, rows)
        for u in range(U):
            gain = out_gain[:, u * Co : (u + 1) * Co]
            result[rows, u * Co : (u + 1) * Co] = ((v[u, rows] - mean) * scale * gain).astype(BF16)

    loop(R, BAND, result_rows)
    sends.drain()


def local(F, T, *args):
    (tokens, query, key, value, lower, decay_up, decay_bias, extra, head_gain, out_weight,
     mix_gain, up, down, out_gain) = args
    U, X = F // T, T // 2
    R, Dt = tokens.shape
    Co = Dt // U
    Rz, kc = query.shape
    W = 2 * kc + value.shape[1]
    Ko = out_weight.shape[0]
    FH = up.shape[1] // 2
    heads = kc // DK
    S, S2, S3 = 2, 2, 2 if Co % (2 * DK) == 0 else 1
    vmem, hbm = pl.BlockSpec(memory_space=pltpu.VMEM), pl.BlockSpec(memory_space=pl.ANY)
    sem = lambda *shape: pltpu.SemaphoreType.DMA(shape)
    buf = lambda *shape: pltpu.VMEM(shape, BF16)
    wide = lambda *shape: pltpu.VMEM(shape, F32)
    H = X * U
    scratch = [
        buf(F, R, Co), buf(F, Rz, W), buf(F, Ko, Co), buf(F, Rz, FH), buf(F, FH, Co),
        buf(R, W), wide(R, kc), buf(R, heads * DV),
        buf(H, R, Co), buf(H, R, Co), buf(H, R, Co), buf(X, U, R, Co), wide(U, R, Co),
        wide(U, R, Co), wide(2, 2, 8, R), wide(2, T, 2, 8, R), buf(2, F, R, Co), buf(2, R, FH),
        buf(H, 2, R, Co), buf(H, 2, R, Co), wide(H, R, Co), buf(H, R, Co), buf(H, R, Co),
        buf(H, R, Co), buf(X, U, R, Co),
        sem(6 + U), sem(T), sem(T), sem(2, F, S), sem(F, S), sem(F, S), sem(F, S),
        sem(2, F), sem(F), sem(F), sem(F),
        sem(F, S2), sem(F, S2), sem(F, S2), sem(F, S2),
        sem(F, S3), sem(F, S3), sem(F, S3), sem(F, S3),
        sem(H), sem(H), sem(H), sem(X, U), sem(2, T), sem(2, T), sem(2, T, X + 1), sem(2, T),
        sem(H, 2, S3), sem(H, 2, S3), sem(H, R // BAND, S3), sem(H, R // BAND, S3),
        sem(H, R // BAND, S3), sem(X, U, R // BAND, S3),
    ]
    return pl.pallas_call(
        functools.partial(kernel, F, T),
        out_shape=jax.ShapeDtypeStruct((R, Dt), BF16),
        in_specs=[hbm, hbm, hbm, hbm, vmem, vmem, vmem, vmem, vmem, hbm, vmem, hbm, hbm, vmem],
        out_specs=vmem,
        scratch_shapes=scratch,
        compiler_params=pltpu.CompilerParams(
            collective_id=0, has_side_effects=True, vmem_limit_bytes=63 * 2**20
        ),
        name="layer",
    )(
        tokens, query, key, value, lower.T, decay_up, decay_bias[None], extra, head_gain[None],
        out_weight, mix_gain[None], up, down, out_gain[None],
    )


def solution(mesh):
    in_specs = (
        P(("grp", "fs"), "tp"),
        P("fs", "tp"),
        P("fs", "tp"),
        P("fs", "tp"),
        P(),
        P(),
        P(),
        P(("grp", "fs"), "tp"),
        P(),
        P("tp", "fs"),
        P("tp"),
        P("fs", "tp"),
        P("tp", "fs"),
        P("tp"),
    )
    out_specs = P(("grp", "fs"), "tp")
    body = functools.partial(local, mesh.shape["fs"], mesh.shape["tp"])
    return jax.shard_map(body, mesh=mesh, in_specs=in_specs, out_specs=out_specs, check_vma=False)
```
